512 devices in a mesh: sp: 128 (over z, y, core), tp: 4 (over x).
Axes of the slice: x: 4, y: 8, z: 8, core: 2. Of those that a mesh axis runs over, the one named last changes fastest.
Arguments:
- glu_value: bfloat16 [131072, 1024], P('sp', 'tp'), may hold values from -6 to 6
- glu_gate: bfloat16 [131072, 1024], P('sp', 'tp'), may hold values from -8 to 8
- conv_taps: float32 [31, 1024], P(None, 'tp'), may hold values from -1 to 1
- channel_gain: float32 [1024], P('tp'), may hold values from 0.1 to 1.9
- proj_weight: bfloat16 [1024, 1024], P('tp'), may hold values from -0.1875 to 0.1875
- out_grad: bfloat16 [131072, 1024], P('sp'), may hold values from -6 to 6
Outputs:
- value_grad: bfloat16 [131072, 1024], P('sp', 'tp')
- gate_grad: bfloat16 [131072, 1024], P('sp', 'tp')
- proj_grad: float32 [1024, 1024], P(('tp', 'sp'))
- taps_grad: float32 [31, 1024], P(None, 'tp')
- norm_gain_gradient: float32 [1024], P('tp')
The draws below stay inside these ranges and needn't reach their ends.
All inputs are finite; a program needn't handle non-finite values.
Results may differ from the reference program's by a relative error of at most 0.0029.
Values may be sent and summed in bfloat16 or wider, within the bound.
A program may use at most 64 MiB of HBM per device.

```python
import jax
import jax.numpy as jnp
from jax import lax

CH = 1024
KERNEL = 31
TOKENS = 131072


def levels(key, shape, split, low, high):
    def one(position, blocks):
        draws = jax.random.uniform(jax.random.fold_in(jax.random.fold_in(key, 6), position), (blocks,), jnp.float32, low / len(split), high / len(split))
        return jnp.repeat(jnp.exp(draws), shape[position] // blocks).reshape((-1,) + (1,) * (len(shape) - position - 1))

    loudness = one(*split[0])
    for cut in split[1:]:
        loudness = loudness * one(*cut)
    return loudness


def centred(stream_key, shape, spread, most, split=(), dtype=jnp.bfloat16):
    entries = spread * jax.random.normal(stream_key, shape, jnp.float32)
    if split:
        entries = entries * levels(stream_key, shape, split, -0.22, 0.18)
    return jnp.clip(entries, -most, most).astype(dtype)


def setup_inputs(seed: int = 0) -> dict:
    key_of = jax.random.split(jax.random.key(seed), 7)
    return {
        "glu_value": centred(key_of[0], (TOKENS, CH), 1.0, 6.0, ((0, 128), (1, 4))),
        "glu_gate": centred(key_of[1], (TOKENS, CH), 1.5, 8.0, ((0, 128), (1, 4))),
        "conv_taps": centred(key_of[2], (KERNEL, CH), KERNEL ** -0.5, 1.0, ((1, 4),), jnp.float32),
        "channel_gain": jnp.clip(1.0 + 0.18 * jax.random.normal(key_of[3], (CH,), jnp.float32), 0.1, 1.9),
        "proj_weight": centred(key_of[4], (CH, CH), CH ** -0.5, 0.1875, ((0, 4),)),
        "out_grad": centred(key_of[5], (TOKENS, CH), 1.0, 6.0, ((0, 128),)),
    }


def reference(glu_value, glu_gate, conv_taps, channel_gain, proj_weight, out_grad):
    halo_rows = KERNEL - 1
    row_count = glu_value.shape[0]
    value_f = glu_value.astype(jnp.float32)
    gate_sig = jax.nn.sigmoid(glu_gate.astype(jnp.float32))
    glu_out = value_f * gate_sig
    padded = jnp.pad(glu_out, ((halo_rows, 0), (0, 0)))
    convolved_output = jnp.zeros_like(glu_out)
    for tap in range(KERNEL):
        convolved_output = convolved_output + conv_taps[tap] * padded[tap:tap + row_count]
    row_average = lax.optimization_barrier(jnp.mean(convolved_output, axis=1, keepdims=True))
    row_sq = lax.optimization_barrier(jnp.mean(convolved_output * convolved_output, axis=1, keepdims=True))
    inverse_deviation = lax.rsqrt(row_sq - row_average * row_average + 1e-05)
    centered_scaled = (convolved_output - row_average) * inverse_deviation
    normalized_rows = centered_scaled * channel_gain
    activ = jax.nn.silu(normalized_rows).astype(jnp.bfloat16)
    act_grad = jnp.dot(out_grad, proj_weight.T, preferred_element_type=jnp.float32)
    norm_sig = jax.nn.sigmoid(normalized_rows)
    normalized_gradient = act_grad * norm_sig * (1.0 + normalized_rows * (1.0 - norm_sig))
    centered_scaled_gradient = normalized_gradient * channel_gain
    convolved_gradient = inverse_deviation * (centered_scaled_gradient - lax.optimization_barrier(jnp.mean(centered_scaled_gradient, axis=1, keepdims=True)) - centered_scaled * lax.optimization_barrier(jnp.mean(centered_scaled_gradient * centered_scaled, axis=1, keepdims=True)))
    gradient_factor = 1.0 / jnp.sqrt(jnp.float32(row_count))
    norm_gain_gradient = lax.optimization_barrier(jnp.sum(normalized_gradient * centered_scaled, axis=0)) * gradient_factor
    taps_grad = jnp.stack([lax.optimization_barrier(jnp.sum(convolved_gradient * padded[tap:tap + row_count], axis=0)) for tap in range(KERNEL)]) * gradient_factor
    grad_pad = jnp.pad(convolved_gradient, ((0, halo_rows), (0, 0)))
    glu_grad = jnp.zeros_like(glu_out)
    for tap in range(KERNEL):
        glu_grad = glu_grad + conv_taps[tap] * grad_pad[halo_rows - tap:halo_rows - tap + row_count]
    value_grad = (glu_grad * gate_sig).astype(jnp.bfloat16)
    gate_grad = (glu_grad * value_f * gate_sig * (1.0 - gate_sig)).astype(jnp.bfloat16)
    proj_grad = jnp.dot(activ.T, out_grad, preferred_element_type=jnp.float32) * gradient_factor
    return (value_grad, gate_grad, proj_grad, taps_grad, norm_gain_gradient)
```

```python
import functools

import jax
import jax.numpy as jnp
from jax import lax
from jax.experimental import pallas as pl
from jax.experimental.pallas import tpu as pltpu
from jax.sharding import Mesh
from jax.sharding import PartitionSpec as P

MESH = pl.DeviceIdType.MESH
SP = ("z", "y", "c")
TP_SP = ("tp", "z", "y", "c")
F32, BF16 = jnp.float32, jnp.bfloat16
HALO = 32
LANES = 128
R = 256
RB = 32


def sigmoid(x):
    return 0.5 * jnp.tanh(0.5 * x) + 0.5


def folded(x):
    return jnp.sum(x.reshape(-1, 8, x.shape[-1]), axis=0)


def kernel(
    sizes,
    value_hbm, gate_hbm, taps_hbm, gain_hbm, w_hbm, og_hbm,
    vg_hbm, gg_hbm, proj_ref, tg_ref, ng_ref,
    value_s, gate_s, taps_s, gain_s, w_s, og_s,
    vh_s, gh_s, glu_s, sig_s, conv_s, xg_s, ag_s, act_s, act_t,
    rcol, mcol, ncol, b1, b2, cg_s, cgh_s, tacc, vg_s, gg_s,
    ex1_src, ex1_rcv, ex2_src, ex2_rcv,
    pc_src, pc_rcv, pz_src, pz_rcv, py_src, py_rcv, ps_src, ps_rcv,
    tc_src, tc_rcv, ta_src, ta_rcv1, ta_rcv2, tb_rcv1, tb_rcv2, ta_mid, ts_src, ts_rcv,
    lsem, hsem, ex1_sem, ex2_sem, cgh_sem, pc_sem, pz_sem, py_sem, ps_sem,
    tc_sem, t1a_sem, t1b_sem, t2a_sem, t2b_sem, ts_sem, osem,
):
    NZ, NY, NTP, T, C, KERNEL, CH, FACTOR = sizes
    NCH = T // R
    SUB = R // LANES
    LT = C // LANES
    z, y, c, x = (lax.axis_index(a) for a in ("z", "y", "c", "tp"))
    sp = (z * NY + y) * 2 + c
    NSP = NZ * NY * 2
    partner = {"c": 1 - c}

    def at_sp(i):
        return {"z": i // (NY * 2), "y": lax.rem(i // 2, NY), "c": lax.rem(i, 2)}

    following, preceding = at_sp(lax.rem(sp + 1, NSP)), at_sp(lax.rem(sp + NSP - 1, NSP))
    tp_peers = [lax.rem(x + d, NTP) for d in range(1, NTP)]
    y_peers = [lax.rem(y + d, NY) for d in range(1, NY)]
    z_peers = [lax.rem(z + d, NZ) for d in range(1, NZ)]

    def remote(src, dst, sems, i, device):
        return pltpu.make_async_remote_copy(
            src_ref=src, dst_ref=dst, send_sem=sems.at[(0, *i)], recv_sem=sems.at[(1, *i)],
            device_id=device, device_id_type=MESH,
        )

    barrier = pltpu.get_barrier_semaphore()
    peers = [partner, following, preceding]
    peers += [{"tp": i} for i in tp_peers] + [{"y": i} for i in y_peers] + [{"z": i} for i in z_peers]

    loads = [
        pltpu.make_async_copy(src, dst, lsem.at[i])
        for i, (src, dst) in enumerate(
            ((value_hbm, value_s), (gate_hbm, gate_s), (taps_hbm, taps_s), (gain_hbm, gain_s), (w_hbm, w_s), (og_hbm, og_s))
        )
    ]
    for copy in loads:
        copy.start()
    for device in peers:
        pl.semaphore_signal(barrier, inc=1, device_id=device, device_id_type=MESH)

    loads[0].wait()
    loads[1].wait()

    def lanes(lt):
        return slice(lt * LANES, (lt + 1) * LANES)

    def glu_block(i, _):
        rows = pl.ds(pl.multiple_of(i * RB, RB), RB)
        into = pl.ds(pl.multiple_of(HALO + i * RB, RB), RB)
        for lt in range(LT):
            s = sigmoid(gate_s[rows, lanes(lt)].astype(F32))
            sig_s[lt, rows, :] = s
            glu_s[lt, into, :] = value_s[rows, lanes(lt)].astype(F32) * s
        return 0

    lax.fori_loop(0, T // RB, glu_block, 0)

    pl.semaphore_wait(barrier, len(peers))
    halo = [
        remote(value_s.at[pl.ds(T - HALO, HALO)], vh_s, hsem, (0,), following),
        remote(gate_s.at[pl.ds(T - HALO, HALO)], gh_s, hsem, (1,), following),
    ]
    for copy in halo:
        copy.start()
    tacc[...] = jnp.zeros_like(tacc)
    loads[2].wait()
    loads[3].wait()

    def ex1(ch, d):
        return remote(ex1_src.at[ch], ex1_rcv.at[ch, x], ex1_sem, (ch, d - 1), {"tp": tp_peers[d - 1]})

    def ex2(ch, d):
        return remote(ex2_src.at[ch], ex2_rcv.at[ch, x], ex2_sem, (ch, d - 1), {"tp": tp_peers[d - 1]})

    def column_sums(blocks):
        return jnp.concatenate(blocks + [jnp.zeros((8 - len(blocks), LANES), F32)], axis=0)

    def stage1(i, _):
        ch = lax.rem(i + 1, NCH)
        first = pl.multiple_of(ch * R, R)

        @pl.when(i == NCH - 1)
        def _():
            for copy in halo:
                copy.wait_recv()
            keep = jnp.where(sp == 0, 0.0, 1.0).astype(F32)
            for lt in range(LT):
                s = sigmoid(gh_s[:, lanes(lt)].astype(F32)) * keep
                glu_s[lt, pl.ds(0, HALO), :] = vh_s[:, lanes(lt)].astype(F32) * s

        for lt in range(LT):

            def conv_block(j, _, lt=lt):
                at = pl.multiple_of(first + j * RB, RB)
                acc = taps_s[0:1, lanes(lt)] * glu_s[lt, pl.ds(at + 2, RB), :]
                for k in range(1, KERNEL):
                    acc += taps_s[k : k + 1, lanes(lt)] * glu_s[lt, pl.ds(at + 2 + k, RB), :]
                conv_s[lt, pl.ds(at, RB), :] = acc
                return 0

            lax.fori_loop(0, R // RB, conv_block, 0)
        sums, squares = [], []
        for s in range(SUB):
            rows = pl.ds(pl.multiple_of(first + s * LANES, LANES), LANES)
            total, square = 0.0, 0.0
            for lt in range(LT):
                v = conv_s[lt, rows, :]
                total, square = total + v, square + v * v
            sums.append(jnp.sum(total.T, axis=0, keepdims=True))
            squares.append(jnp.sum(square.T, axis=0, keepdims=True))
        block = column_sums(sums + squares)
        ex1_src[ch] = block
        ex1_rcv[ch, x] = block
        for d in range(1, NTP):
            ex1(ch, d).start()
        return 0

    lax.fori_loop(0, NCH, stage1, 0)

    loads[4].wait()
    loads[5].wait()

    def act_grad_block(i, _):
        rows = pl.ds(pl.multiple_of(i * R, R), R)
        g = lax.dot_general(
            og_s[rows, :], w_s[...], (((1,), (1,)), ((), ())), preferred_element_type=F32
        )
        for lt in range(LT):
            ag_s[lt, rows, :] = g[:, lanes(lt)]
        return 0

    lax.fori_loop(0, NCH, act_grad_block, 0)

    def column(row):
        return jnp.broadcast_to(row, (LANES, LANES)).T

    def stage2(i, _):
        ch = lax.rem(i + 1, NCH)
        first = pl.multiple_of(ch * R, R)
        for d in range(1, NTP):
            ex1(ch, d).wait()
        total = ex1_rcv[ch, 0]
        for t in range(1, NTP):
            total += ex1_rcv[ch, t]
        total = total * (1.0 / CH)
        mean = total[0:SUB]
        inv = lax.rsqrt(total[SUB : 2 * SUB] - mean * mean + 1e-05)
        for s in range(SUB):
            rows = pl.ds(pl.multiple_of(first + s * LANES, LANES), LANES)
            mcol[rows, :] = column(mean[s : s + 1])
            rcol[rows, :] = column(inv[s : s + 1])

        def norm_block(j, carry):
            rows = pl.ds(pl.multiple_of(first + j * RB, RB), RB)
            local = pl.ds(pl.multiple_of(j * RB, RB), RB)
            m, r = mcol[rows, :], rcol[rows, :]
            s1, s2, gains = 0.0, 0.0, []
            for lt in range(LT):
                gain = gain_s[0:1, lanes(lt)]
                xhat = (conv_s[lt, rows, :] - m) * r
                n = xhat * gain
                s = sigmoid(n)
                act_s[local, lanes(lt)] = (n * s).astype(BF16)
                ng = ag_s[lt, rows, :] * (s * (1.0 + n * (1.0 - s)))
                xg = ng * gain
                conv_s[lt, rows, :] = xhat
                xg_s[lt, rows, :] = xg
                s1, s2 = s1 + xg, s2 + xg * xhat
                gains.append(carry[lt] + folded(ng * xhat))
            b1[local, :] = s1
            b2[local, :] = s2
            return tuple(gains)

        gains = lax.fori_loop(
            0, R // RB, norm_block, tuple(jnp.zeros((8, LANES), F32) for _ in range(LT))
        )
        for lt in range(LT):
            tacc[lt, KERNEL] += gains[lt]
        blocks = [
            jnp.sum(b[s * LANES : (s + 1) * LANES, :].T, axis=0, keepdims=True)
            for b in (b1, b2)
            for s in range(SUB)
        ]
        block = column_sums(blocks)
        ex2_src[ch] = block
        ex2_rcv[ch, x] = block
        for d in range(1, NTP):
            ex2(ch, d).start()
        for lt in range(LT):
            for s in range(SUB):
                at = pl.ds(pl.multiple_of(first + s * LANES, LANES), LANES)
                act_t[lanes(lt), at] = act_s[s * LANES : (s + 1) * LANES, lanes(lt)].T
        return 0

    lax.fori_loop(0, NCH, stage2, 0)

    D = og_s.shape[1]
    H = D // 2

    def partial(owner):
        columns = pl.ds(pl.multiple_of(owner * H, H), H)
        return jnp.dot(act_t[...], og_s[:, columns], preferred_element_type=F32)

    pc_src[...] = (partial(1 - c) * FACTOR).astype(BF16)
    core_copy = remote(pc_src, pc_rcv, pc_sem, (), partner)
    core_copy.start()
    own_partial = partial(c) * FACTOR
    core_copy.wait()
    own_partial = own_partial + pc_rcv[...].astype(F32)
    ZB = C // NZ
    for i in range(NZ):
        pz_src[i] = own_partial[i * ZB : (i + 1) * ZB].astype(BF16)
    pz = [
        remote(pz_src.at[z_peers[d - 1]], pz_rcv.at[z], pz_sem, (d - 1,), {"z": z_peers[d - 1]})
        for d in range(1, NZ)
    ]
    for copy in pz:
        copy.start()
    pz_rcv[z] = pz_src[z]

    cgh = remote(cg_s.at[:, pl.ds(0, HALO), :], cgh_s, cgh_sem, (), preceding)

    def stage3(ch, _):
        first = pl.multiple_of(ch * R, R)
        for d in range(1, NTP):
            ex2(ch, d).wait()
        total = ex2_rcv[ch, 0]
        for t in range(1, NTP):
            total += ex2_rcv[ch, t]
        total = total * (1.0 / CH)
        for s in range(SUB):
            rows = pl.ds(pl.multiple_of(first + s * LANES, LANES), LANES)
            mcol[rows, :] = column(total[s : s + 1])
            ncol[rows, :] = column(total[SUB + s : SUB + s + 1])
        for lt in range(LT):

            def taps_block(j, carry, lt=lt):
                at = pl.multiple_of(first + j * RB, RB)
                rows = pl.ds(at, RB)
                g = rcol[rows, :] * (
                    xg_s[lt, rows, :] - mcol[rows, :] - conv_s[lt, rows, :] * ncol[rows, :]
                )
                cg_s[lt, rows, :] = g
                return tuple(
                    carry[k] + folded(g * glu_s[lt, pl.ds(at + 2 + k, RB), :])
                    for k in range(KERNEL)
                )

            sums = lax.fori_loop(
                0, R // RB, taps_block, tuple(jnp.zeros((8, LANES), F32) for _ in range(KERNEL))
            )
            for k in range(KERNEL):
                tacc[lt, k] += sums[k]

        @pl.when(ch == 0)
        def _():
            cgh.start()

        return 0

    lax.fori_loop(0, NCH, stage3, 0)

    for lt in range(LT):
        tc_src[lt] = jnp.sum(tacc[lt], axis=1) * FACTOR
    taps_core = remote(tc_src.at[1 - c], tc_rcv, tc_sem, (), partner)
    taps_core.start()

    def back_block(j, _):
        at = pl.multiple_of(j * RB, RB)
        rows = pl.ds(at, RB)
        for lt in range(LT):
            acc = taps_s[KERNEL - 1 : KERNEL, lanes(lt)] * cg_s[lt, rows, :]
            for k in range(1, KERNEL):
                tap = KERNEL - 1 - k
                acc += taps_s[tap : tap + 1, lanes(lt)] * cg_s[lt, pl.ds(at + k, RB), :]
            s = sig_s[lt, rows, :]
            glu = glu_s[lt, pl.ds(pl.multiple_of(at + HALO, RB), RB), :]
            vg_s[rows, lanes(lt)] = (acc * s).astype(BF16)
            gg_s[rows, lanes(lt)] = (acc * glu * (1.0 - s)).astype(BF16)
        return 0

    PER = R // RB

    def stage4(ch):
        lax.fori_loop(ch * PER, (ch + 1) * PER, back_block, 0)
        rows = pl.ds(ch * R, R)
        outs = [
            pltpu.make_async_copy(vg_s.at[rows], vg_hbm.at[rows], osem.at[ch, 0]),
            pltpu.make_async_copy(gg_s.at[rows], gg_hbm.at[rows], osem.at[ch, 1]),
        ]
        for copy in outs:
            copy.start()
        return outs

    stores = []
    stores += stage4(0)

    taps_core.wait()
    S = KERNEL + 1
    A = S // 2
    both = tc_src[c] + tc_rcv[...]
    ta_src[0] = both[0:A]
    ta_src[1] = both[A:S]
    first_hops = [
        remote(ta_src.at[0], ta_rcv1.at[y], t1a_sem, (d - 1,), {"y": y_peers[d - 1]}) for d in range(1, NY)
    ] + [
        remote(ta_src.at[1], tb_rcv1.at[z], t1b_sem, (d - 1,), {"z": z_peers[d - 1]}) for d in range(1, NZ)
    ]
    for copy in first_hops:
        copy.start()
    ta_rcv1[y] = both[0:A]
    tb_rcv1[z] = both[A:S]

    for ch in range(1, NCH - 1):
        stores += stage4(ch)
    cgh.wait()
    last = jnp.where(sp == NSP - 1, 0.0, 1.0).astype(F32)
    cg_s[:, pl.ds(T, HALO), :] = cgh_s[...] * last
    stores += stage4(NCH - 1)

    def summed(ref, n):
        total = ref[0].astype(F32)
        for i in range(1, n):
            total += ref[i].astype(F32)
        return total

    for copy in first_hops:
        copy.wait()
    half_a, half_b = summed(ta_rcv1, NY), summed(tb_rcv1, NZ)
    ta_mid[0] = half_a
    ta_mid[1] = half_b
    second_hops = [
        remote(ta_mid.at[0], ta_rcv2.at[z], t2a_sem, (d - 1,), {"z": z_peers[d - 1]}) for d in range(1, NZ)
    ] + [
        remote(ta_mid.at[1], tb_rcv2.at[y], t2b_sem, (d - 1,), {"y": y_peers[d - 1]}) for d in range(1, NY)
    ]
    for copy in second_hops:
        copy.start()
    ta_rcv2[z] = half_a
    tb_rcv2[y] = half_b

    for copy in pz:
        copy.wait()
    rows_z = summed(pz_rcv, NZ)
    YB = ZB // NY
    for i in range(NY):
        py_src[i] = rows_z[i * YB : (i + 1) * YB]
    py = [
        remote(py_src.at[y_peers[d - 1]], py_rcv.at[y], py_sem, (d - 1,), {"y": y_peers[d - 1]})
        for d in range(1, NY)
    ]
    for copy in py:
        copy.start()
    py_rcv[y] = py_src[y]

    for copy in second_hops:
        copy.wait()
    ts_src[0:A] = summed(ta_rcv2, NZ)
    ts_src[A:S] = summed(tb_rcv2, NY)
    taps_swap = remote(ts_src, ts_rcv, ts_sem, (), partner)
    taps_swap.start()

    for copy in py:
        copy.wait()
    rows_y = summed(py_rcv, NY)
    CB = YB // 2
    for i in range(2):
        ps_src[i] = rows_y[i * CB : (i + 1) * CB]
    proj_swap = remote(ps_src.at[1 - c], ps_rcv, ps_sem, (), partner)
    proj_swap.start()

    taps_swap.wait()
    mine, theirs = ts_src[...], ts_rcv[...]
    for lt in range(LT):
        v = jnp.where(c == lt, mine, theirs)
        tg_ref[:, lanes(lt)] = v[0:KERNEL]
        ng_ref[:, lanes(lt)] = v[KERNEL : KERNEL + 1]
    proj_swap.wait()
    mine, theirs = ps_src[c], ps_rcv[...]
    for i in range(2):
        proj_ref[:, i * H : (i + 1) * H] = jnp.where(c == i, mine, theirs)
    for copy in halo:
        copy.wait_send()
    for copy in stores:
        copy.wait()


def per_device(sizes, glu_value, glu_gate, conv_taps, channel_gain, proj_weight, out_grad):
    NZ, NY, NTP = sizes
    T, C = glu_value.shape
    K = conv_taps.shape[0]
    D = out_grad.shape[1]
    NCH, LT, S, A = T // R, C // LANES, K + 1, (K + 1) // 2
    ZB = C // NZ
    YB = ZB // NY
    CB = YB // 2
    H = D // 2
    factor = float(1.0 / (T * NZ * NY * 2) ** 0.5)
    params = (NZ, NY, NTP, T, C, K, C * NTP, factor)
    full = (LT, T, LANES)
    vmem, dma = pltpu.VMEM, pltpu.SemaphoreType.DMA
    any_spec = pl.BlockSpec(memory_space=pl.ANY)
    vmem_spec = pl.BlockSpec(memory_space=pltpu.VMEM)
    scratch = [
        vmem((T, C), BF16), vmem((T, C), BF16), vmem((K, C), F32), vmem((1, C), F32),
        vmem((C, D), BF16), vmem((T, D), BF16),
        vmem((HALO, C), BF16), vmem((HALO, C), BF16),
        vmem((LT, T + HALO, LANES), F32), vmem(full, F32), vmem(full, F32), vmem(full, F32), vmem(full, F32),
        vmem((R, C), BF16), vmem((C, T), BF16),
        vmem((T, LANES), F32), vmem((T, LANES), F32), vmem((T, LANES), F32),
        vmem((R, LANES), F32), vmem((R, LANES), F32),
        vmem((LT, T + HALO, LANES), F32), vmem((LT, HALO, LANES), F32),
        vmem((LT, S, 8, LANES), F32), vmem((T, C), BF16), vmem((T, C), BF16),
        vmem((NCH, 8, LANES), F32), vmem((NCH, NTP, 8, LANES), F32),
        vmem((NCH, 8, LANES), F32), vmem((NCH, NTP, 8, LANES), F32),
        vmem((C, H), BF16), vmem((C, H), BF16),
        vmem((NZ, ZB, H), BF16), vmem((NZ, ZB, H), BF16),
        vmem((NY, YB, H), F32), vmem((NY, YB, H), F32),
        vmem((2, CB, H), F32), vmem((CB, H), F32),
        vmem((LT, S, LANES), F32), vmem((S, LANES), F32),
        vmem((2, A, LANES), F32),
        vmem((NY, A, LANES), F32), vmem((NZ, A, LANES), F32),
        vmem((NZ, A, LANES), F32), vmem((NY, A, LANES), F32),
        vmem((2, A, LANES), F32), vmem((S, LANES), F32), vmem((S, LANES), F32),
        dma((6,)), dma((2, 2)), dma((2, NCH, NTP - 1)), dma((2, NCH, NTP - 1)), dma((2,)),
        dma((2,)), dma((2, NZ - 1)), dma((2, NY - 1)), dma((2,)),
        dma((2,)), dma((2, NY - 1)), dma((2, NZ - 1)), dma((2, NZ - 1)), dma((2, NY - 1)), dma((2,)),
        dma((NCH, 2)),
    ]
    value_grad, gate_grad, proj_grad, taps_grad, gain_grad = pl.pallas_call(
        functools.partial(kernel, params),
        out_shape=(
            jax.ShapeDtypeStruct((T, C), BF16),
            jax.ShapeDtypeStruct((T, C), BF16),
            jax.ShapeDtypeStruct((CB, D), F32),
            jax.ShapeDtypeStruct((K, C), F32),
            jax.ShapeDtypeStruct((1, C), F32),
        ),
        in_specs=[any_spec] * 6,
        out_specs=(any_spec, any_spec, vmem_spec, vmem_spec, vmem_spec),
        scratch_shapes=scratch,
        compiler_params=pltpu.CompilerParams(
            collective_id=0, has_side_effects=True, vmem_limit_bytes=60 * 2**20
        ),
    )(glu_value, glu_gate, conv_taps, channel_gain[None], proj_weight, out_grad)
    return value_grad, gate_grad, proj_grad, taps_grad, gain_grad[0]


def solution(mesh):
    return sized(mesh, 8, 8)


def sized(mesh, nz, ny):
    tp = mesh.shape["tp"]
    finer = Mesh(mesh.devices.reshape(nz, ny, 2, tp), ("z", "y", "c", "tp"))
    return jax.shard_map(
        functools.partial(per_device, (nz, ny, tp)),
        mesh=finer,
        in_specs=(P(SP, "tp"), P(SP, "tp"), P(None, "tp"), P("tp"), P("tp", None), P(SP, None)),
        out_specs=(P(SP, "tp"), P(SP, "tp"), P(TP_SP, None), P(None, "tp"), P("tp")),
        check_vma=False,
    )
```

```python
import functools

import jax
import jax.numpy as jnp
from jax import lax
from jax.experimental import pallas as pl
from jax.experimental.pallas import tpu as pltpu
from jax.sharding import Mesh
from jax.sharding import PartitionSpec as P

MESH = pl.DeviceIdType.MESH
SP = ("z", "y", "c")
TP_SP = ("tp", "z", "y", "c")
F32, BF16 = jnp.float32, jnp.bfloat16
HALO = 32
LANES = 128
R = 256
RB = 32
GB = 64
VB = 64
NB = 32
TB = 64


def sigmoid(x):
    return 0.5 * jnp.tanh(0.5 * x) + 0.5


def folded(x):
    return jnp.sum(x.reshape(-1, 8, x.shape[-1]), axis=0)


def kernel(
    sizes,
    value_hbm, gate_hbm, taps_hbm, gain_hbm, w_hbm, og_hbm,
    vg_ref, gg_ref, proj_ref, tg_ref, ng_ref,
    value_s, gate_s, taps_s, gain_s, w_s, og_s,
    vh_s, gh_s, glu_s, sig_s, conv_s, xg_s, ag_s, act_s, act_t, act_p,
    rcol, mcol, ncol, b1, b2, cg_s, cgh_s, tacc,
    ex1_src, ex1_rcv, ex2_src, ex2_rcv,
    pc_src, pc_rcv, own_s, pa_src, pa_rcv, pb_src, pb_rcv, qa_src, qa_rcv, qb_src, qb_rcv, ps_src, ps_rcv,
    tc_src, tc_rcv, ta_src, ta_rcv1, ta_rcv2, tb_rcv1, tb_rcv2, ta_mid, ts_src, ts_rcv,
    lsem, hsem, ex1_sem, ex2_sem, cgh_sem, pc_sem, pa_sem, pb_sem, qa_sem, qb_sem, ps_sem,
    tc_sem, t1a_sem, t1b_sem, t2a_sem, t2b_sem, ts_sem,
):
    NZ, NY, NTP, T, C, KERNEL, CH, FACTOR = sizes
    NCH = T // R
    SUB = R // LANES
    LT = C // LANES
    z, y, c, x = (lax.axis_index(a) for a in ("z", "y", "c", "tp"))
    sp = (z * NY + y) * 2 + c
    NSP = NZ * NY * 2
    partner = {"c": 1 - c}

    def at_sp(i):
        return {"z": i // (NY * 2), "y": lax.rem(i // 2, NY), "c": lax.rem(i, 2)}

    following, preceding = at_sp(lax.rem(sp + 1, NSP)), at_sp(lax.rem(sp + NSP - 1, NSP))
    tp_peers = [lax.rem(x + d, NTP) for d in range(1, NTP)]
    y_peers = [lax.rem(y + d, NY) for d in range(1, NY)]
    z_peers = [lax.rem(z + d, NZ) for d in range(1, NZ)]

    def remote(src, dst, sems, i, device):
        return pltpu.make_async_remote_copy(
            src_ref=src, dst_ref=dst, send_sem=sems.at[(0, *i)], recv_sem=sems.at[(1, *i)],
            device_id=device, device_id_type=MESH,
        )

    barrier = pltpu.get_barrier_semaphore()
    peers = [partner, following, preceding]
    peers += [{"tp": i} for i in tp_peers] + [{"y": i} for i in y_peers] + [{"z": i} for i in z_peers]

    loads = [
        pltpu.make_async_copy(src, dst, lsem.at[i])
        for i, (src, dst) in enumerate(
            ((value_hbm, value_s), (gate_hbm, gate_s), (taps_hbm, taps_s), (gain_hbm, gain_s), (w_hbm, w_s), (og_hbm, og_s))
        )
    ]
    for copy in loads:
        copy.start()
    for device in peers:
        pl.semaphore_signal(barrier, inc=1, device_id=device, device_id_type=MESH)

    loads[0].wait()
    loads[1].wait()

    def lanes(lt):
        return slice(lt * LANES, (lt + 1) * LANES)

    def glu_block(i, _):
        rows = pl.ds(pl.multiple_of(i * GB, GB), GB)
        into = pl.ds(pl.multiple_of(HALO + i * GB, HALO), GB)
        for lt in range(LT):
            s = sigmoid(gate_s[rows, lanes(lt)].astype(F32))
            sig_s[lt, rows, :] = s
            glu_s[lt, into, :] = value_s[rows, lanes(lt)].astype(F32) * s
        return 0

    lax.fori_loop(0, T // GB, glu_block, 0)

    pl.semaphore_wait(barrier, len(peers))
    halo = [
        remote(value_s.at[pl.ds(T - HALO, HALO)], vh_s, hsem, (0,), following),
        remote(gate_s.at[pl.ds(T - HALO, HALO)], gh_s, hsem, (1,), following),
    ]
    for copy in halo:
        copy.start()
    tacc[...] = jnp.zeros_like(tacc)
    loads[2].wait()
    loads[3].wait()

    def ex1(ch, d):
        return remote(ex1_src.at[ch], ex1_rcv.at[ch, x], ex1_sem, (ch, d - 1), {"tp": tp_peers[d - 1]})

    def ex2(ch, d):
        return remote(ex2_src.at[ch], ex2_rcv.at[ch, x], ex2_sem, (ch, d - 1), {"tp": tp_peers[d - 1]})

    def column_sums(blocks):
        return jnp.concatenate(blocks + [jnp.zeros((8 - len(blocks), LANES), F32)], axis=0)

    def stage1(i, _):
        ch = lax.rem(i + 1, NCH)
        first = pl.multiple_of(ch * R, R)

        @pl.when(i == NCH - 1)
        def _():
            for copy in halo:
                copy.wait_recv()
            keep = jnp.where(sp == 0, 0.0, 1.0).astype(F32)
            for lt in range(LT):
                s = sigmoid(gh_s[:, lanes(lt)].astype(F32)) * keep
                glu_s[lt, pl.ds(0, HALO), :] = vh_s[:, lanes(lt)].astype(F32) * s

        for lt in range(LT):

            def conv_block(j, _, lt=lt):
                at = pl.multiple_of(first + j * VB, VB)
                acc = taps_s[0:1, lanes(lt)] * glu_s[lt, pl.ds(at + 2, VB), :]
                for k in range(1, KERNEL):
                    acc += taps_s[k : k + 1, lanes(lt)] * glu_s[lt, pl.ds(at + 2 + k, VB), :]
                conv_s[lt, pl.ds(at, VB), :] = acc
                return 0

            lax.fori_loop(0, R // VB, conv_block, 0)
        sums, squares = [], []
        for s in range(SUB):
            rows = pl.ds(pl.multiple_of(first + s * LANES, LANES), LANES)
            total, square = 0.0, 0.0
            for lt in range(LT):
                v = conv_s[lt, rows, :]
                total, square = total + v, square + v * v
            sums.append(jnp.sum(total.T, axis=0, keepdims=True))
            squares.append(jnp.sum(square.T, axis=0, keepdims=True))
        block = column_sums(sums + squares)
        ex1_src[ch] = block
        ex1_rcv[ch, x] = block
        for d in range(1, NTP):
            ex1(ch, d).start()
        return 0

    lax.fori_loop(0, NCH, stage1, 0)

    loads[4].wait()
    loads[5].wait()

    def act_grad_block(i, _):
        rows = pl.ds(pl.multiple_of(i * R, R), R)
        g = lax.dot_general(
            og_s[rows, :], w_s[...], (((1,), (1,)), ((), ())), preferred_element_type=F32
        )
        for lt in range(LT):
            ag_s[lt, rows, :] = g[:, lanes(lt)]
        return 0

    lax.fori_loop(0, NCH, act_grad_block, 0)

    def column(row):
        return jnp.broadcast_to(row, (LANES, LANES)).T

    def stage2(i, _):
        ch = lax.rem(i + 1, NCH)
        first = pl.multiple_of(ch * R, R)
        for d in range(1, NTP):
            ex1(ch, d).wait()
        total = ex1_rcv[ch, 0]
        for t in range(1, NTP):
            total += ex1_rcv[ch, t]
        total = total * (1.0 / CH)
        mean = total[0:SUB]
        inv = lax.rsqrt(total[SUB : 2 * SUB] - mean * mean + 1e-05)
        for s in range(SUB):
            rows = pl.ds(pl.multiple_of(first + s * LANES, LANES), LANES)
            mcol[rows, :] = column(mean[s : s + 1])
            rcol[rows, :] = column(inv[s : s + 1])

        def norm_block(j, carry):
            rows = pl.ds(pl.multiple_of(first + j * NB, NB), NB)
            local = pl.ds(pl.multiple_of(j * NB, NB), NB)
            m, r = mcol[rows, :], rcol[rows, :]
            s1, s2, gains = 0.0, 0.0, []
            for lt in range(LT):
                gain = gain_s[0:1, lanes(lt)]
                xhat = (conv_s[lt, rows, :] - m) * r
                n = xhat * gain
                s = sigmoid(n)
                act_s[local, lanes(lt)] = (n * s).astype(BF16)
                ng = ag_s[lt, rows, :] * (s * (1.0 + n * (1.0 - s)))
                xg = ng * gain
                conv_s[lt, rows, :] = xhat
                xg_s[lt, rows, :] = xg
                s1, s2 = s1 + xg, s2 + xg * xhat
                gains.append(carry[lt] + folded(ng * xhat))
            b1[local, :] = s1
            b2[local, :] = s2
            return tuple(gains)

        gains = lax.fori_loop(
            0, R // NB, norm_block, tuple(jnp.zeros((8, LANES), F32) for _ in range(LT))
        )
        for lt in range(LT):
            tacc[lt, KERNEL] += gains[lt]
        blocks = [
            jnp.sum(b[s * LANES : (s + 1) * LANES, :].T, axis=0, keepdims=True)
            for b in (b1, b2)
            for s in range(SUB)
        ]
        block = column_sums(blocks)
        ex2_src[ch] = block
        ex2_rcv[ch, x] = block
        for d in range(1, NTP):
            ex2(ch, d).start()
        for lt in range(LT):
            for s in range(SUB):
                at = pl.ds(pl.multiple_of(first + s * LANES, LANES), LANES)
                act_t[lanes(lt), at] = act_s[s * LANES : (s + 1) * LANES, lanes(lt)].T
        return 0

    lax.fori_loop(0, NCH - 1, stage2, 0)

    cgh = remote(cg_s.at[:, pl.ds(0, HALO), :], cgh_s, cgh_sem, (), preceding)

    def stage3(ch):
        first = ch * R
        for d in range(1, NTP):
            ex2(ch, d).wait()
        total = ex2_rcv[ch, 0]
        for t in range(1, NTP):
            total += ex2_rcv[ch, t]
        total = total * (1.0 / CH)
        for s in range(SUB):
            rows = pl.ds(first + s * LANES, LANES)
            mcol[rows, :] = column(total[s : s + 1])
            ncol[rows, :] = column(total[SUB + s : SUB + s + 1])
        for lt in range(LT):

            def taps_block(j, carry, lt=lt):
                at = pl.multiple_of(first + j * TB, TB)
                rows = pl.ds(at, TB)
                g = rcol[rows, :] * (
                    xg_s[lt, rows, :] - mcol[rows, :] - conv_s[lt, rows, :] * ncol[rows, :]
                )
                cg_s[lt, rows, :] = g
                return tuple(
                    carry[k] + folded(g * glu_s[lt, pl.ds(at + 2 + k, TB), :])
                    for k in range(KERNEL)
                )

            sums = lax.fori_loop(
                0, R // TB, taps_block, tuple(jnp.zeros((8, LANES), F32) for _ in range(KERNEL))
            )
            for k in range(KERNEL):
                tacc[lt, k] += sums[k]

    def back_block(j, _):
        at = pl.multiple_of(j * RB, RB)
        rows = pl.ds(at, RB)
        for lt in range(LT):
            acc = taps_s[KERNEL - 1 : KERNEL, lanes(lt)] * cg_s[lt, rows, :]
            for k in range(1, KERNEL):
                tap = KERNEL - 1 - k
                acc += taps_s[tap : tap + 1, lanes(lt)] * cg_s[lt, pl.ds(at + k, RB), :]
            s = sig_s[lt, rows, :]
            glu = glu_s[lt, pl.ds(pl.multiple_of(at + HALO, RB), RB), :]
            vg_ref[rows, lanes(lt)] = (acc * s).astype(BF16)
            gg_ref[rows, lanes(lt)] = (acc * glu * (1.0 - s)).astype(BF16)
        return 0

    PER = R // RB

    def stage4(ch):
        lax.fori_loop(ch * PER, (ch + 1) * PER, back_block, 0)

    def summed(ref, n):
        total = ref[0].astype(F32)
        for i in range(1, n):
            total += ref[i].astype(F32)
        return total

    order = [(i + 1) % NCH for i in range(NCH)]
    stage3(order[0])
    stage2(NCH - 1, 0)

    D = og_s.shape[1]
    H = D // 2
    Q = H // 2
    B = C // (NZ * NY)
    shape = (C, C)
    i = lax.broadcasted_iota(jnp.int32, shape, 0)
    j = lax.broadcasted_iota(jnp.int32, shape, 1)
    source = ((i // B) % NZ) * (NY * B) + (i // (B * NZ)) * B + i % B
    permutation = jnp.where(j == source, 1.0, 0.0).astype(BF16)
    act_p[...] = jnp.dot(permutation, act_t[...], preferred_element_type=F32).astype(BF16)

    def partial(owner, part):
        columns = pl.ds(pl.multiple_of(owner * H + part * Q, Q), Q)
        rows = (act_t, act_p)[part]
        return jnp.dot(rows[...], og_s[:, columns], preferred_element_type=F32) * FACTOR

    for part in range(2):
        pc_src[part] = partial(1 - c, part).astype(BF16)
    core_copy = remote(pc_src, pc_rcv, pc_sem, (), partner)
    core_copy.start()
    for part in range(2):
        own_s[part] = partial(c, part)

    stage3(order[1])

    core_copy.wait()
    ZB, YB = C // NZ, C // NY
    own = own_s[0] + pc_rcv[0].astype(F32)
    for i in range(NZ):
        pa_src[i] = own[i * ZB : (i + 1) * ZB].astype(BF16)
    own = own_s[1] + pc_rcv[1].astype(F32)
    for i in range(NY):
        pb_src[i] = own[i * YB : (i + 1) * YB].astype(BF16)

    def to_z(src, dst, sems):
        return [
            remote(src.at[z_peers[d - 1]], dst.at[z], sems, (d - 1,), {"z": z_peers[d - 1]}) for d in range(1, NZ)
        ]

    def to_y(src, dst, sems):
        return [
            remote(src.at[y_peers[d - 1]], dst.at[y], sems, (d - 1,), {"y": y_peers[d - 1]}) for d in range(1, NY)
        ]

    proj_first = to_z(pa_src, pa_rcv, pa_sem) + to_y(pb_src, pb_rcv, pb_sem)
    for copy in proj_first:
        copy.start()
    pa_rcv[z] = pa_src[z]
    pb_rcv[y] = pb_src[y]

    for ch in order[2:-1]:
        stage3(ch)
    stage4(order[0])
    stage3(0)
    cgh.start()

    S = KERNEL + 1
    A = S // 2
    for lt in range(LT):
        tc_src[:, lanes(lt)] = jnp.sum(tacc[lt], axis=1) * FACTOR
    taps_core = remote(tc_src, tc_rcv, tc_sem, (), partner)
    taps_first = [
        remote(ta_src.at[0], ta_rcv1.at[y], t1a_sem, (d - 1,), {"y": y_peers[d - 1]}) for d in range(1, NY)
    ] + [
        remote(ta_src.at[1], tb_rcv1.at[z], t1b_sem, (d - 1,), {"z": z_peers[d - 1]}) for d in range(1, NZ)
    ]
    taps_second = [
        remote(ta_mid.at[0], ta_rcv2.at[z], t2a_sem, (d - 1,), {"z": z_peers[d - 1]}) for d in range(1, NZ)
    ] + [
        remote(ta_mid.at[1], tb_rcv2.at[y], t2b_sem, (d - 1,), {"y": y_peers[d - 1]}) for d in range(1, NY)
    ]
    taps_swap = remote(ts_src, ts_rcv, ts_sem, (), partner)

    @pl.when(c == 0)
    def _():
        taps_core.start()

    stage4(0)

    @pl.when(c == 1)
    def _():
        taps_core.wait_recv()
        both = tc_src[...] + tc_rcv[...]
        ta_src[0] = both[0:A]
        ta_src[1] = both[A:S]
        for copy in taps_first:
            copy.start()
        ta_rcv1[y] = both[0:A]
        tb_rcv1[z] = both[A:S]

    for ch in order[1:-2]:
        stage4(ch)
    cgh.wait()
    last = jnp.where(sp == NSP - 1, 0.0, 1.0).astype(F32)
    cg_s[:, pl.ds(T, HALO), :] = cgh_s[...] * last
    stage4(NCH - 1)

    for copy in proj_first:
        copy.wait()
    part_a, part_b = summed(pa_rcv, NZ), summed(pb_rcv, NY)
    for i in range(NY):
        qa_src[i] = part_a[i * B : (i + 1) * B]
    for i in range(NZ):
        qb_src[i] = part_b[i * B : (i + 1) * B]
    proj_second = to_y(qa_src, qa_rcv, qa_sem) + to_z(qb_src, qb_rcv, qb_sem)
    for copy in proj_second:
        copy.start()
    qa_rcv[y] = qa_src[y]
    qb_rcv[z] = qb_src[z]

    @pl.when(c == 1)
    def _():
        for copy in taps_first:
            copy.wait()
        half_a, half_b = summed(ta_rcv1, NY), summed(tb_rcv1, NZ)
        ta_mid[0] = half_a
        ta_mid[1] = half_b
        for copy in taps_second:
            copy.start()
        ta_rcv2[z] = half_a
        tb_rcv2[y] = half_b

    for copy in proj_second:
        copy.wait()
    done_a, done_b = summed(qa_rcv, NY), summed(qb_rcv, NZ)
    CB = B // 2
    for i in range(2):
        ps_src[i, :, 0:Q] = done_a[i * CB : (i + 1) * CB]
        ps_src[i, :, Q:H] = done_b[i * CB : (i + 1) * CB]
    proj_swap = remote(ps_src.at[1 - c], ps_rcv, ps_sem, (), partner)
    proj_swap.start()

    @pl.when(c == 1)
    def _():
        for copy in taps_second:
            copy.wait()
        ts_src[0:A] = summed(ta_rcv2, NZ)
        ts_src[A:S] = summed(tb_rcv2, NY)
        taps_swap.start()
        tg_ref[...] = ts_src[0:KERNEL]
        ng_ref[...] = ts_src[KERNEL : KERNEL + 1]

    proj_swap.wait()
    mine, theirs = ps_src[c], ps_rcv[...]
    for i in range(2):
        proj_ref[:, i * H : (i + 1) * H] = jnp.where(c == i, mine, theirs)
    for copy in halo:
        copy.wait_send()

    @pl.when(c == 1)
    def _():
        taps_swap.wait_send()

    @pl.when(c == 0)
    def _():
        taps_core.wait_send()
        taps_swap.wait_recv()
        tg_ref[...] = ts_rcv[0:KERNEL]
        ng_ref[...] = ts_rcv[KERNEL : KERNEL + 1]


def store_kernel(*refs):
    n = len(refs) // 2
    sems = refs[-1]
    copies = [pltpu.make_async_copy(refs[i], refs[n + i], sems.at[i]) for i in range(n)]
    for copy in copies:
        copy.start()
    for copy in copies:
        copy.wait()


def per_device(sizes, glu_value, glu_gate, conv_taps, channel_gain, proj_weight, out_grad):
    NZ, NY, NTP = sizes
    T, C = glu_value.shape
    K = conv_taps.shape[0]
    D = out_grad.shape[1]
    NCH, LT, S, A = T // R, C // LANES, K + 1, (K + 1) // 2
    ZB, YB, B = C // NZ, C // NY, C // (NZ * NY)
    CB = B // 2
    H, Q = D // 2, D // 4
    factor = float(1.0 / (T * NZ * NY * 2) ** 0.5)
    params = (NZ, NY, NTP, T, C, K, C * NTP, factor)
    full = (LT, T, LANES)
    vmem, dma = pltpu.VMEM, pltpu.SemaphoreType.DMA
    any_spec = pl.BlockSpec(memory_space=pltpu.HBM)
    vmem_spec = pl.BlockSpec(memory_space=pltpu.VMEM)
    scratch = [
        vmem((T, C), BF16), vmem((T, C), BF16), vmem((K, C), F32), vmem((1, C), F32),
        vmem((C, D), BF16), vmem((T, D), BF16),
        vmem((HALO, C), BF16), vmem((HALO, C), BF16),
        vmem((LT, T + HALO, LANES), F32), vmem(full, F32), vmem(full, F32), vmem(full, F32), vmem(full, F32),
        vmem((R, C), BF16), vmem((C, T), BF16), vmem((C, T), BF16),
        vmem((T, LANES), F32), vmem((T, LANES), F32), vmem((T, LANES), F32),
        vmem((R, LANES), F32), vmem((R, LANES), F32),
        vmem((LT, T + HALO, LANES), F32), vmem((LT, HALO, LANES), F32),
        vmem((LT, S, 8, LANES), F32),
        vmem((NCH, 8, LANES), F32), vmem((NCH, NTP, 8, LANES), F32),
        vmem((NCH, 8, LANES), F32), vmem((NCH, NTP, 8, LANES), F32),
        vmem((2, C, Q), BF16), vmem((2, C, Q), BF16), vmem((2, C, Q), F32),
        vmem((NZ, ZB, Q), BF16), vmem((NZ, ZB, Q), BF16),
        vmem((NY, YB, Q), BF16), vmem((NY, YB, Q), BF16),
        vmem((NY, B, Q), F32), vmem((NY, B, Q), F32),
        vmem((NZ, B, Q), F32), vmem((NZ, B, Q), F32),
        vmem((2, CB, H), F32), vmem((CB, H), F32),
        vmem((S, C), F32), vmem((S, C), F32),
        vmem((2, A, C), F32),
        vmem((NY, A, C), F32), vmem((NZ, A, C), F32),
        vmem((NZ, A, C), F32), vmem((NY, A, C), F32),
        vmem((2, A, C), F32), vmem((S, C), F32), vmem((S, C), F32),
        dma((6,)), dma((2, 2)), dma((2, NCH, NTP - 1)), dma((2, NCH, NTP - 1)), dma((2,)),
        dma((2,)), dma((2, NZ - 1)), dma((2, NY - 1)), dma((2, NY - 1)), dma((2, NZ - 1)), dma((2,)),
        dma((2,)), dma((2, NY - 1)), dma((2, NZ - 1)), dma((2, NZ - 1)), dma((2, NY - 1)), dma((2,)),
    ]
    results = (
        jax.ShapeDtypeStruct((T, C), BF16),
        jax.ShapeDtypeStruct((T, C), BF16),
        jax.ShapeDtypeStruct((CB, D), F32),
        jax.ShapeDtypeStruct((K, C), F32),
        jax.ShapeDtypeStruct((1, C), F32),
    )
    held = pl.pallas_call(
        functools.partial(kernel, params),
        out_shape=results,
        in_specs=[any_spec] * 6,
        out_specs=(vmem_spec,) * 5,
        scratch_shapes=scratch,
        compiler_params=pltpu.CompilerParams(
            collective_id=0, has_side_effects=True, vmem_limit_bytes=40 * 2**20
        ),
    )(*(
        pltpu.with_memory_space_constraint(a, pltpu.HBM)
        for a in (glu_value, glu_gate, conv_taps, channel_gain[None], proj_weight, out_grad)
    ))
    value_grad, gate_grad, proj_grad, taps_grad, gain_grad = pl.pallas_call(
        store_kernel,
        out_shape=results,
        in_specs=[vmem_spec] * 5,
        out_specs=(any_spec,) * 5,
        scratch_shapes=[dma((5,))],
        compiler_params=pltpu.CompilerParams(vmem_limit_bytes=8 * 2**20),
    )(*held)
    return value_grad, gate_grad, proj_grad, taps_grad, gain_grad[0]


def solution(mesh):
    return sized(mesh, 8, 8)


def sized(mesh, nz, ny):
    tp = mesh.shape["tp"]
    finer = Mesh(mesh.devices.reshape(nz, ny, 2, tp), ("z", "y", "c", "tp"))
    return jax.shard_map(
        functools.partial(per_device, (nz, ny, tp)),
        mesh=finer,
        in_specs=(P(SP, "tp"), P(SP, "tp"), P(None, "tp"), P("tp"), P("tp", None), P(SP, None)),
        out_specs=(P(SP, "tp"), P(SP, "tp"), P(TP_SP, None), P(None, "tp"), P("tp")),
        check_vma=False,
    )
```

```python
import functools

import jax
import jax.numpy as jnp
from jax import lax
from jax.experimental import pallas as pl
from jax.experimental.pallas import tpu as pltpu
from jax.sharding import Mesh
from jax.sharding import PartitionSpec as P

MESH = pl.DeviceIdType.MESH
SP = ("z", "y", "c")
TP_SP = ("tp", "z", "y", "c")
F32, BF16 = jnp.float32, jnp.bfloat16
HALO = 32
LANES = 128
R = 256
RB = 32
GB = 64
VB = 64
NB = 32
TB = 64
AB = 512


def sigmoid(x):
    return 0.5 * jnp.tanh(0.5 * x) + 0.5


def folded(x):
    return jnp.sum(x.reshape(-1, 8, x.shape[-1]), axis=0)


def kernel(
    sizes,
    value_hbm, gate_hbm, taps_hbm, gain_hbm, w_hbm, og_hbm,
    vg_ref, gg_ref, proj_ref, tg_ref, ng_ref,
    value_s, gate_s, taps_s, gain_s, w_s, og_s,
    hv_s, glu_s, sig_s, conv_s, xg_s, ag_s, act_s, act_t, act_p,
    rcol, mcol, ncol, b1, b2, cg_s, cgh_s, tacc,
    ex1_src, ex1_rcv, ex2_src, ex2_rcv,
    pc_src, pc_rcv, own_s, p1_src, p1_rcv, p2_src, p2_rcv, ps_src, ps_rcv,
    tc_src, tc_rcv, t1_src, t1_rcv, t2_src, t2_rcv, ts_src, ts_rcv,
    lsem, hsem, ex1_sem, ex2_sem, cgh_sem, pc_sem, p1_sem, p2_sem, ps_sem, tc_sem, t1_sem, t2_sem, ts_sem,
):
    NZ, NY, NTP, T, C, KERNEL, CH, FACTOR = sizes
    NBLK = T // LANES
    BIG = (T - 2 * LANES) // R
    chunks = [(LANES + i * R, R) for i in range(BIG)] + [(T - LANES, LANES), (0, LANES)]
    LT = C // LANES
    z, y, c, x = (lax.axis_index(a) for a in ("z", "y", "c", "tp"))
    sp = (z * NY + y) * 2 + c
    NSP = NZ * NY * 2
    partner = {"c": 1 - c}

    def at_sp(i):
        return {"z": i // (NY * 2), "y": lax.rem(i // 2, NY), "c": lax.rem(i, 2)}

    following, preceding = at_sp(lax.rem(sp + 1, NSP)), at_sp(lax.rem(sp + NSP - 1, NSP))
    tp_peers = [lax.rem(x + d, NTP) for d in range(1, NTP)]
    y_peers = [lax.rem(y + d, NY) for d in range(1, NY)]
    z_peers = [lax.rem(z + d, NZ) for d in range(1, NZ)]

    def remote(src, dst, sems, device, i=0):
        return pltpu.make_async_remote_copy(
            src_ref=src, dst_ref=dst, send_sem=sems.at[0], recv_sem=sems.at[1 + i],
            device_id=device, device_id_type=MESH,
        )

    barrier = pltpu.get_barrier_semaphore()
    peers = [partner, following, preceding]
    peers += [{"tp": i} for i in tp_peers] + [{"y": i} for i in y_peers] + [{"z": i} for i in z_peers]

    loads = [
        pltpu.make_async_copy(src, dst, lsem.at[i])
        for i, (src, dst) in enumerate(
            ((value_hbm, value_s), (gate_hbm, gate_s), (taps_hbm, taps_s), (gain_hbm, gain_s), (w_hbm, w_s), (og_hbm, og_s))
        )
    ]
    for copy in loads:
        copy.start()
    for device in peers:
        pl.semaphore_signal(barrier, inc=1, device_id=device, device_id_type=MESH)

    loads[0].wait()
    loads[1].wait()

    def lanes(lt):
        return slice(lt * LANES, (lt + 1) * LANES)

    def glu_block(i, _):
        rows = pl.ds(pl.multiple_of(i * GB, GB), GB)
        into = pl.ds(pl.multiple_of(HALO + i * GB, HALO), GB)
        for lt in range(LT):
            s = sigmoid(gate_s[rows, lanes(lt)].astype(F32))
            sig_s[lt, rows, :] = s
            glu_s[lt, into, :] = value_s[rows, lanes(lt)].astype(F32) * s
        return 0

    lax.fori_loop(0, T // GB, glu_block, 0)

    pl.semaphore_wait(barrier, len(peers))
    tail = pl.ds(T - HALO, HALO)
    remote(value_s.at[tail], hv_s.at[0], hsem, following).start()
    remote(gate_s.at[tail], hv_s.at[1], hsem, following).start()
    halo = remote(hv_s, hv_s, hsem, following)
    tacc[...] = jnp.zeros_like(tacc)
    loads[2].wait()
    loads[3].wait()

    def exchange(src, rcv, sem, n):
        first, size = chunks[n]
        blocks = pl.ds(first // LANES, size // LANES)
        for peer in tp_peers:
            remote(src.at[blocks], rcv.at[x, blocks], sem, {"tp": peer}, n).start()

    def received(rcv, sem, block, count, n):
        sample = rcv.at[pl.ds(0, NTP - 1), pl.ds(block, count)]
        remote(sample, sample, sem, partner, n).wait_recv()

    def record(src, rcv, block, rows):
        for i, row in enumerate(rows):
            src[block, i : i + 1, :] = row
            rcv[x, block, i : i + 1, :] = row

    def row_sums(v):
        return jnp.sum(v.T, axis=0, keepdims=True)

    def conv_stats(block):
        rows = pl.ds(pl.multiple_of(block * LANES, LANES), LANES)
        total, square = 0.0, 0.0
        for lt in range(LT):
            v = conv_s[lt, rows, :]
            total, square = total + v, square + v * v
        return row_sums(total), row_sums(square)

    def conv_block(block):
        for lt in range(LT):
            for half in range(LANES // VB):
                at = pl.multiple_of(block * LANES + half * VB, VB)
                acc = taps_s[0:1, lanes(lt)] * glu_s[lt, pl.ds(at + 2, VB), :]
                for k in range(1, KERNEL):
                    acc += taps_s[k : k + 1, lanes(lt)] * glu_s[lt, pl.ds(at + 2 + k, VB), :]
                conv_s[lt, pl.ds(at, VB), :] = acc

    conv_block(1)

    def stage1(block, _):
        sums = conv_stats(block)

        conv_block(lax.rem(block + 1, NBLK))
        record(ex1_src, ex1_rcv, block, sums)
        for n, (first, size) in enumerate(chunks[:-1]):

            @pl.when(block == (first + size) // LANES - 1)
            def _(n=n):
                exchange(ex1_src, ex1_rcv, ex1_sem, n)

        @pl.when(block == NBLK - 2)
        def _():
            halo.wait_recv()
            keep = jnp.where(sp == 0, 0.0, 1.0).astype(F32)
            for lt in range(LT):
                s = sigmoid(hv_s[1, :, lanes(lt)].astype(F32)) * keep
                glu_s[lt, pl.ds(0, HALO), :] = hv_s[0, :, lanes(lt)].astype(F32) * s

        return 0

    lax.fori_loop(1, NBLK, stage1, 0)
    record(ex1_src, ex1_rcv, 0, conv_stats(0))
    exchange(ex1_src, ex1_rcv, ex1_sem, len(chunks) - 1)

    loads[4].wait()
    loads[5].wait()

    def act_grad_block(i, _):
        rows = pl.ds(pl.multiple_of(i * AB, AB), AB)
        g = lax.dot_general(
            og_s[rows, :], w_s[...], (((1,), (1,)), ((), ())), preferred_element_type=F32
        )
        for lt in range(LT):
            ag_s[lt, rows, :] = g[:, lanes(lt)]
        return 0

    lax.fori_loop(0, T // AB, act_grad_block, 0)

    def column(row):
        return jnp.broadcast_to(row, (LANES, LANES)).T

    def totals(rcv, sem, block, count, n):
        received(rcv, sem, block, count, n)
        both = []
        for s in range(count):
            total = rcv[0, block + s]
            for t in range(1, NTP):
                total += rcv[t, block + s]
            both.append(total * (1.0 / CH))
        return both

    def stage2(n, first, size):
        block, count = first // LANES, size // LANES
        for s, total in enumerate(totals(ex1_rcv, ex1_sem, block, count, n)):
            mean = total[0:1]
            inv = lax.rsqrt(total[1:2] - mean * mean + 1e-05)
            rows = pl.ds(pl.multiple_of(first + s * LANES, LANES), LANES)
            mcol[rows, :] = column(mean)
            rcol[rows, :] = column(inv)

        def norm_block(j, carry):
            rows = pl.ds(pl.multiple_of(first + j * NB, NB), NB)
            local = pl.ds(pl.multiple_of(j * NB, NB), NB)
            m, r = mcol[rows, :], rcol[rows, :]
            s1, s2, gains = 0.0, 0.0, []
            for lt in range(LT):
                gain = gain_s[0:1, lanes(lt)]
                xhat = (conv_s[lt, rows, :] - m) * r
                n = xhat * gain
                s = sigmoid(n)
                act_s[local, lanes(lt)] = (n * s).astype(BF16)
                ng = ag_s[lt, rows, :] * (s * (1.0 + n * (1.0 - s)))
                xg = ng * gain
                conv_s[lt, rows, :] = xhat
                xg_s[lt, rows, :] = xg
                s1, s2 = s1 + xg, s2 + xg * xhat
                gains.append(carry[lt] + folded(ng * xhat))
            b1[local, :] = s1
            b2[local, :] = s2
            return tuple(gains)

        gains = lax.fori_loop(
            0, size // NB, norm_block, tuple(jnp.zeros((8, LANES), F32) for _ in range(LT))
        )
        for lt in range(LT):
            tacc[lt, KERNEL] += gains[lt]
        for s in range(count):
            part = slice(s * LANES, (s + 1) * LANES)
            record(ex2_src, ex2_rcv, block + s, (row_sums(b1[part, :]), row_sums(b2[part, :])))
        for peer in tp_peers:
            blocks = pl.ds(block, count)
            remote(ex2_src.at[blocks], ex2_rcv.at[x, blocks], ex2_sem, {"tp": peer}, n).start()
        for lt in range(LT):
            for s in range(count):
                at = pl.ds(pl.multiple_of(first + s * LANES, LANES), LANES)
                act_t[lanes(lt), at] = act_s[s * LANES : (s + 1) * LANES, lanes(lt)].T

    def stage2_big(i, _):
        stage2(i, pl.multiple_of(LANES + i * R, LANES), R)
        return 0

    lax.fori_loop(0, BIG, stage2_big, 0)
    stage2(BIG, *chunks[BIG])
    stage2(BIG + 1, *chunks[BIG + 1])

    cgh = remote(cg_s.at[:, pl.ds(0, HALO), :], cgh_s, cgh_sem, preceding)

    def stage3(n):
        first, size = chunks[n]
        block, count = first // LANES, size // LANES
        for s, total in enumerate(totals(ex2_rcv, ex2_sem, block, count, n)):
            rows = pl.ds(first + s * LANES, LANES)
            mcol[rows, :] = column(total[0:1])
            ncol[rows, :] = column(total[1:2])
        for lt in range(LT):

            def taps_block(j, carry, lt=lt):
                at = pl.multiple_of(first + j * TB, TB)
                rows = pl.ds(at, TB)
                g = rcol[rows, :] * (
                    xg_s[lt, rows, :] - mcol[rows, :] - conv_s[lt, rows, :] * ncol[rows, :]
                )
                cg_s[lt, rows, :] = g
                return tuple(
                    carry[k] + folded(g * glu_s[lt, pl.ds(at + 2 + k, TB), :])
                    for k in range(KERNEL)
                )

            sums = lax.fori_loop(
                0, size // TB, taps_block, tuple(jnp.zeros((8, LANES), F32) for _ in range(KERNEL))
            )
            for k in range(KERNEL):
                tacc[lt, k] += sums[k]

    def back_block(j, _):
        at = pl.multiple_of(j * RB, RB)
        rows = pl.ds(at, RB)
        for lt in range(LT):
            acc = taps_s[KERNEL - 1 : KERNEL, lanes(lt)] * cg_s[lt, rows, :]
            for k in range(1, KERNEL):
                tap = KERNEL - 1 - k
                acc += taps_s[tap : tap + 1, lanes(lt)] * cg_s[lt, pl.ds(at + k, RB), :]
            s = sig_s[lt, rows, :]
            glu = glu_s[lt, pl.ds(pl.multiple_of(at + HALO, RB), RB), :]
            vg_ref[rows, lanes(lt)] = (acc * s).astype(BF16)
            gg_ref[rows, lanes(lt)] = (acc * glu * (1.0 - s)).astype(BF16)
        return 0

    def stage4(first, last):
        lax.fori_loop(first // RB, last // RB, back_block, 0)

    def summed(ref, n):
        total = ref[0].astype(F32)
        for i in range(1, n):
            total += ref[i].astype(F32)
        return total

    D = og_s.shape[1]
    H = D // 2
    Q = H // 2
    B = C // (NZ * NY)
    shape = (C, C)
    i = lax.broadcasted_iota(jnp.int32, shape, 0)
    j = lax.broadcasted_iota(jnp.int32, shape, 1)
    source = ((i // B) % NZ) * (NY * B) + (i // (B * NZ)) * B + i % B
    permutation = jnp.where(j == source, 1.0, 0.0).astype(BF16)
    act_p[...] = jnp.dot(permutation, act_t[...], preferred_element_type=F32).astype(BF16)

    def partial(owner, part):
        columns = pl.ds(pl.multiple_of(owner * H + part * Q, Q), Q)
        rows = (act_t, act_p)[part]
        return jnp.dot(rows[...], og_s[:, columns], preferred_element_type=F32) * FACTOR

    for part in range(2):
        pc_src[part] = partial(1 - c, part).astype(BF16)
    core_copy = remote(pc_src, pc_rcv, pc_sem, partner)
    core_copy.start()
    for part in range(2):
        own_s[part] = partial(c, part)

    stage3(0)

    core_copy.wait()
    N = NZ
    ZB = C // N

    def both_ways(src, dst, sems, swapped):
        z_part, y_part = (1, 0) if swapped else (0, 1)
        for i in z_peers:
            remote(src(z_part, i), dst.at[z_part, z], sems, {"z": i}).start()
        for i in y_peers:
            remote(src(y_part, i), dst.at[y_part, y], sems, {"y": i}).start()

    def finish(dst, sems):
        sample = dst.at[:, pl.ds(0, N - 1)]
        remote(sample, sample, sems, partner).wait()

    for part in range(2):
        own = own_s[part] + pc_rcv[part].astype(F32)
        for i in range(N):
            p1_src[part, i] = own[i * ZB : (i + 1) * ZB].astype(BF16)
    both_ways(lambda part, i: p1_src.at[part, i], p1_rcv, p1_sem, False)
    p1_rcv[0, z] = p1_src[0, z]
    p1_rcv[1, y] = p1_src[1, y]

    for n in range(1, len(chunks)):
        stage3(n)
    cgh.start()

    S = KERNEL + 1
    A = S // 2
    for lt in range(LT):
        tc_src[:, lanes(lt)] = jnp.sum(tacc[lt], axis=1) * FACTOR
    taps_core = remote(tc_src, tc_rcv, tc_sem, partner)
    taps_swap = remote(ts_src, ts_rcv, ts_sem, partner)

    @pl.when(c == 0)
    def _():
        taps_core.start()

    stage4(0, R)

    @pl.when(c == 1)
    def _():
        taps_core.wait_recv()
        both = tc_src[...] + tc_rcv[...]
        t1_src[0] = both[0:A]
        t1_src[1] = both[A:S]
        both_ways(lambda part, i: t1_src.at[part], t1_rcv, t1_sem, False)
        t1_rcv[0, z] = both[0:A]
        t1_rcv[1, y] = both[A:S]

    stage4(R, T - R)
    cgh.wait()
    last = jnp.where(sp == NSP - 1, 0.0, 1.0).astype(F32)
    cg_s[:, pl.ds(T, HALO), :] = cgh_s[...] * last
    stage4(T - R, T)

    finish(p1_rcv, p1_sem)
    for part in range(2):
        sums = summed(p1_rcv.at[part], N)
        for i in range(N):
            p2_src[part, i] = sums[i * B : (i + 1) * B]
    both_ways(lambda part, i: p2_src.at[part, i], p2_rcv, p2_sem, True)
    p2_rcv[0, y] = p2_src[0, y]
    p2_rcv[1, z] = p2_src[1, z]

    @pl.when(c == 1)
    def _():
        finish(t1_rcv, t1_sem)
        half_a, half_b = summed(t1_rcv.at[0], N), summed(t1_rcv.at[1], N)
        t2_src[0] = half_a
        t2_src[1] = half_b
        both_ways(lambda part, i: t2_src.at[part], t2_rcv, t2_sem, True)
        t2_rcv[0, y] = half_a
        t2_rcv[1, z] = half_b

    finish(p2_rcv, p2_sem)
    done_a, done_b = summed(p2_rcv.at[0], N), summed(p2_rcv.at[1], N)
    CB = B // 2
    for i in range(2):
        ps_src[i, :, 0:Q] = done_a[i * CB : (i + 1) * CB]
        ps_src[i, :, Q:H] = done_b[i * CB : (i + 1) * CB]
    proj_swap = remote(ps_src.at[1 - c], ps_rcv, ps_sem, partner)
    proj_swap.start()

    @pl.when(c == 1)
    def _():
        finish(t2_rcv, t2_sem)
        ts_src[0:A] = summed(t2_rcv.at[0], N)
        ts_src[A:S] = summed(t2_rcv.at[1], N)
        taps_swap.start()
        tg_ref[...] = ts_src[0:KERNEL]
        ng_ref[...] = ts_src[KERNEL : KERNEL + 1]

    proj_swap.wait()
    mine, theirs = ps_src[c], ps_rcv[...]
    for i in range(2):
        proj_ref[:, i * H : (i + 1) * H] = jnp.where(c == i, mine, theirs)
    halo.wait_send()
    for rcv, sem in ((ex1_rcv, ex1_sem), (ex2_rcv, ex2_sem)):
        sample = rcv.at[pl.ds(0, NTP - 1)]
        remote(sample, sample, sem, partner).wait_send()

    @pl.when(c == 1)
    def _():
        taps_swap.wait_send()

    @pl.when(c == 0)
    def _():
        taps_core.wait_send()
        taps_swap.wait_recv()
        tg_ref[...] = ts_rcv[0:KERNEL]
        ng_ref[...] = ts_rcv[KERNEL : KERNEL + 1]


def store_kernel(*refs):
    n = len(refs) // 2
    sems = refs[-1]
    copies = [pltpu.make_async_copy(refs[i], refs[n + i], sems.at[i]) for i in range(n)]
    for copy in copies:
        copy.start()
    for copy in copies:
        copy.wait()


def per_device(sizes, glu_value, glu_gate, conv_taps, channel_gain, proj_weight, out_grad):
    NZ, NY, NTP = sizes
    T, C = glu_value.shape
    K = conv_taps.shape[0]
    D = out_grad.shape[1]
    LT, S, A = C // LANES, K + 1, (K + 1) // 2
    N, ZB, B = NZ, C // NZ, C // (NZ * NY)
    NBLK = T // LANES
    NCH = (T - 2 * LANES) // R + 2
    CB = B // 2
    H, Q = D // 2, D // 4
    factor = float(1.0 / (T * NZ * NY * 2) ** 0.5)
    params = (NZ, NY, NTP, T, C, K, C * NTP, factor)
    full = (LT, T, LANES)
    vmem, dma = pltpu.VMEM, pltpu.SemaphoreType.DMA
    any_spec = pl.BlockSpec(memory_space=pltpu.HBM)
    vmem_spec = pl.BlockSpec(memory_space=pltpu.VMEM)
    scratch = [
        vmem((T, C), BF16), vmem((T, C), BF16), vmem((K, C), F32), vmem((1, C), F32),
        vmem((C, D), BF16), vmem((T, D), BF16),
        vmem((2, HALO, C), BF16),
        vmem((LT, T + HALO, LANES), F32), vmem(full, F32), vmem(full, F32), vmem(full, F32), vmem(full, F32),
        vmem((R, C), BF16), vmem((C, T), BF16), vmem((C, T), BF16),
        vmem((T, LANES), F32), vmem((T, LANES), F32), vmem((T, LANES), F32),
        vmem((R, LANES), F32), vmem((R, LANES), F32),
        vmem((LT, T + HALO, LANES), F32), vmem((LT, HALO, LANES), F32),
        vmem((LT, S, 8, LANES), F32),
        vmem((NBLK, 2, LANES), F32), vmem((NTP, NBLK, 2, LANES), F32),
        vmem((NBLK, 2, LANES), F32), vmem((NTP, NBLK, 2, LANES), F32),
        vmem((2, C, Q), BF16), vmem((2, C, Q), BF16), vmem((2, C, Q), F32),
        vmem((2, N, ZB, Q), BF16), vmem((2, N, ZB, Q), BF16),
        vmem((2, N, B, Q), F32), vmem((2, N, B, Q), F32),
        vmem((2, CB, H), F32), vmem((CB, H), F32),
        vmem((S, C), F32), vmem((S, C), F32),
        vmem((2, A, C), F32), vmem((2, N, A, C), F32),
        vmem((2, A, C), F32), vmem((2, N, A, C), F32),
        vmem((S, C), F32), vmem((S, C), F32),
        dma((6,)), dma((2,)), dma((1 + NCH,)), dma((1 + NCH,)), dma((2,)),
    ] + [dma((2,))] * 8 + [
    ]
    results = (
        jax.ShapeDtypeStruct((T, C), BF16),
        jax.ShapeDtypeStruct((T, C), BF16),
        jax.ShapeDtypeStruct((CB, D), F32),
        jax.ShapeDtypeStruct((K, C), F32),
        jax.ShapeDtypeStruct((1, C), F32),
    )
    held = pl.pallas_call(
        functools.partial(kernel, params),
        out_shape=results,
        in_specs=[any_spec] * 6,
        out_specs=(vmem_spec,) * 5,
        scratch_shapes=scratch,
        compiler_params=pltpu.CompilerParams(
            collective_id=0, has_side_effects=True, vmem_limit_bytes=40 * 2**20
        ),
    )(*(
        pltpu.with_memory_space_constraint(a, pltpu.HBM)
        for a in (glu_value, glu_gate, conv_taps, channel_gain[None], proj_weight, out_grad)
    ))
    value_grad, gate_grad, proj_grad, taps_grad, gain_grad = pl.pallas_call(
        store_kernel,
        out_shape=results,
        in_specs=[vmem_spec] * 5,
        out_specs=(any_spec,) * 5,
        scratch_shapes=[dma((5,))],
        compiler_params=pltpu.CompilerParams(vmem_limit_bytes=8 * 2**20),
    )(*held)
    return value_grad, gate_grad, proj_grad, taps_grad, gain_grad[0]


def solution(mesh):
    return sized(mesh, 8, 8)


def sized(mesh, nz, ny):
    tp = mesh.shape["tp"]
    finer = Mesh(mesh.devices.reshape(nz, ny, 2, tp), ("z", "y", "c", "tp"))
    return jax.shard_map(
        functools.partial(per_device, (nz, ny, tp)),
        mesh=finer,
        in_specs=(P(SP, "tp"), P(SP, "tp"), P(None, "tp"), P("tp"), P("tp", None), P(SP, None)),
        out_specs=(P(SP, "tp"), P(SP, "tp"), P(TP_SP, None), P(None, "tp"), P("tp")),
        check_vma=False,
    )
```

```python
import functools

import jax
import jax.numpy as jnp
from jax import lax
from jax.experimental import pallas as pl
from jax.experimental.pallas import tpu as pltpu
from jax.sharding import Mesh
from jax.sharding import PartitionSpec as P

MESH = pl.DeviceIdType.MESH
SP = ("z", "y", "c")
TP_SP = ("tp", "z", "y", "c")
F32, BF16 = jnp.float32, jnp.bfloat16
HALO = 32
LANES = 128
R = 256
RB = 32
GB = 64
VB = 64
NB = 32
TB = 64
AB = 512


def sigmoid(x):
    return 0.5 * jnp.tanh(0.5 * x) + 0.5


def folded(x):
    return jnp.sum(x.reshape(-1, 8, x.shape[-1]), axis=0)


def kernel(
    sizes,
    value_hbm, gate_hbm, taps_hbm, gain_hbm, w_hbm, og_hbm,
    vg_ref, gg_ref, proj_ref, tg_ref, ng_ref,
    value_s, gate_s, taps_s, gain_s, w_s, og_s,
    hv_s, glu_s, sig_s, conv_s, xg_s, ag_s, act_t, act_p,
    rcol, mcol, ncol, cg_s, cgh_s, tacc,
    ex1_src, ex1_rcv, ex2_src, ex2_rcv,
    pc_src, pc_rcv, own_s, p1_src, p1_rcv, p2_src, p2_rcv, ps_src, ps_rcv,
    tc_src, tc_rcv, t1_src, t1_rcv, t2_src, t2_rcv, ts_src, ts_rcv,
    lsem, hsem, ex1_sem, ex2_sem, cgh_sem, pc_sem, p1_sem, p2_sem, ps_sem, tc_sem, t1_sem, t2_sem, ts_sem,
):
    NZ, NY, NTP, T, C, KERNEL, CH, FACTOR = sizes
    NBLK = T // LANES
    BIG = (T - 2 * LANES) // R
    chunks = [(LANES + i * R, R) for i in range(BIG)] + [(T - LANES, LANES), (0, LANES)]
    LT = C // LANES
    z, y, c, x = (lax.axis_index(a) for a in ("z", "y", "c", "tp"))
    sp = (z * NY + y) * 2 + c
    NSP = NZ * NY * 2
    partner = {"c": 1 - c}

    def at_sp(i):
        return {"z": i // (NY * 2), "y": lax.rem(i // 2, NY), "c": lax.rem(i, 2)}

    following, preceding = at_sp(lax.rem(sp + 1, NSP)), at_sp(lax.rem(sp + NSP - 1, NSP))

    def others(i, n):
        return [lax.rem(i + d, n) for d in sorted(range(1, n), key=lambda d: -min(d, n - d))]

    tp_peers, y_peers, z_peers = others(x, NTP), others(y, NY), others(z, NZ)

    def remote(src, dst, sems, device, i=0):
        return pltpu.make_async_remote_copy(
            src_ref=src, dst_ref=dst, send_sem=sems.at[0], recv_sem=sems.at[1 + i],
            device_id=device, device_id_type=MESH,
        )

    barrier = pltpu.get_barrier_semaphore()
    peers = [partner, following, preceding]
    peers += [{"tp": i} for i in tp_peers] + [{"y": i} for i in y_peers] + [{"z": i} for i in z_peers]

    loads = [
        pltpu.make_async_copy(src, dst, lsem.at[i])
        for i, (src, dst) in enumerate(
            ((value_hbm, value_s), (gate_hbm, gate_s), (taps_hbm, taps_s), (gain_hbm, gain_s), (w_hbm, w_s), (og_hbm, og_s))
        )
    ]
    for copy in loads:
        copy.start()
    for device in peers:
        pl.semaphore_signal(barrier, inc=1, device_id=device, device_id_type=MESH)

    loads[0].wait()
    loads[1].wait()

    def lanes(lt):
        return slice(lt * LANES, (lt + 1) * LANES)

    def glu_block(i, _):
        rows = pl.ds(pl.multiple_of(i * GB, GB), GB)
        into = pl.ds(pl.multiple_of(HALO + i * GB, HALO), GB)
        for lt in range(LT):
            s = sigmoid(gate_s[rows, lanes(lt)].astype(F32))
            sig_s[lt, rows, :] = s
            glu_s[lt, into, :] = value_s[rows, lanes(lt)].astype(F32) * s
        return 0

    lax.fori_loop(0, T // GB, glu_block, 0)

    pl.semaphore_wait(barrier, len(peers))
    tail = pl.ds(T - HALO, HALO)
    remote(value_s.at[tail], hv_s.at[0], hsem, following).start()
    remote(gate_s.at[tail], hv_s.at[1], hsem, following).start()
    halo = remote(hv_s, hv_s, hsem, following)
    tacc[...] = jnp.zeros_like(tacc)
    loads[2].wait()
    loads[3].wait()

    def exchange(src, rcv, sem, n):
        first, size = chunks[n]
        blocks = pl.ds(first // LANES, size // LANES)
        for peer in tp_peers:
            remote(src.at[blocks], rcv.at[x, blocks], sem, {"tp": peer}, n).start()

    def received(rcv, sem, block, count, n):
        sample = rcv.at[pl.ds(0, NTP - 1), pl.ds(block, count)]
        remote(sample, sample, sem, partner, n).wait_recv()

    def record(src, rcv, block, rows):
        for i, row in enumerate(rows):
            src[block, i : i + 1, :] = row
            rcv[x, block, i : i + 1, :] = row

    def row_sums(v):
        return jnp.sum(v.T, axis=0, keepdims=True)

    def windows(ref, lt, at, size):
        for s in range(8):
            steps = len(range(s, KERNEL, 8))
            wide = ref[lt, pl.ds(at + s, size + 8 * (steps - 1)), :]
            for m in range(steps):
                yield s + 8 * m, wide[8 * m : 8 * m + size]

    def conv_stats(block):
        rows = pl.ds(pl.multiple_of(block * LANES, LANES), LANES)
        total, square = 0.0, 0.0
        for lt in range(LT):
            v = conv_s[lt, rows, :]
            total, square = total + v, square + v * v
        return row_sums(total), row_sums(square)

    def conv_block(block):
        for lt in range(LT):
            for half in range(LANES // VB):
                at = pl.multiple_of(block * LANES + half * VB, VB)
                acc = jnp.zeros((VB, LANES), F32)
                for k, window in windows(glu_s, lt, at + 2, VB):
                    acc += taps_s[k : k + 1, lanes(lt)] * window
                conv_s[lt, pl.ds(at, VB), :] = acc

    conv_block(1)

    def stage1(block, _):
        sums = conv_stats(block)

        conv_block(lax.rem(block + 1, NBLK))
        record(ex1_src, ex1_rcv, block, sums)
        for n, (first, size) in enumerate(chunks[:-1]):

            @pl.when(block == (first + size) // LANES - 1)
            def _(n=n):
                exchange(ex1_src, ex1_rcv, ex1_sem, n)

        @pl.when(block == NBLK - 2)
        def _():
            halo.wait_recv()
            keep = jnp.where(sp == 0, 0.0, 1.0).astype(F32)
            for lt in range(LT):
                s = sigmoid(hv_s[1, :, lanes(lt)].astype(F32)) * keep
                glu_s[lt, pl.ds(0, HALO), :] = hv_s[0, :, lanes(lt)].astype(F32) * s

        return 0

    lax.fori_loop(1, NBLK, stage1, 0)
    record(ex1_src, ex1_rcv, 0, conv_stats(0))
    exchange(ex1_src, ex1_rcv, ex1_sem, len(chunks) - 1)

    loads[4].wait()
    loads[5].wait()

    def act_grad_block(i, _):
        rows = pl.ds(pl.multiple_of(i * AB, AB), AB)
        g = lax.dot_general(
            og_s[rows, :], w_s[...], (((1,), (1,)), ((), ())), preferred_element_type=F32
        )
        for lt in range(LT):
            ag_s[lt, rows, :] = g[:, lanes(lt)]
        return 0

    lax.fori_loop(0, T // AB, act_grad_block, 0)

    def column(row):
        return jnp.broadcast_to(row, (LANES, LANES)).T

    def totals(rcv, sem, block, count, n):
        received(rcv, sem, block, count, n)
        both = []
        for s in range(count):
            total = rcv[0, block + s]
            for t in range(1, NTP):
                total += rcv[t, block + s]
            both.append(total * (1.0 / CH))
        return both

    def stage2(n, first, size):
        block, count = first // LANES, size // LANES
        activ = []
        for s, total in enumerate(totals(ex1_rcv, ex1_sem, block, count, n)):
            mean = total[0:1]
            inv = lax.rsqrt(total[1:2] - mean * mean + 1e-05)
            m, r = column(mean), column(inv)
            start = first + s * LANES
            rcol[pl.ds(pl.multiple_of(start, LANES), LANES), :] = r
            sums1, sums2, acts = [], [], [[] for _ in range(LT)]
            gains = [0.0] * LT
            for j in range(0, LANES, NB):
                rows = pl.ds(pl.multiple_of(start + j, NB), NB)
                s1, s2 = 0.0, 0.0
                for lt in range(LT):
                    gain = gain_s[0:1, lanes(lt)]
                    xhat = (conv_s[lt, rows, :] - m[j : j + NB]) * r[j : j + NB]
                    n_ = xhat * gain
                    g = sigmoid(n_)
                    acts[lt].append((n_ * g).astype(BF16))
                    ng = ag_s[lt, rows, :] * (g * (1.0 + n_ * (1.0 - g)))
                    xg = ng * gain
                    conv_s[lt, rows, :] = xhat
                    xg_s[lt, rows, :] = xg
                    s1, s2 = s1 + xg, s2 + xg * xhat
                    gains[lt] += folded(ng * xhat)
                sums1.append(s1)
                sums2.append(s2)
            for lt in range(LT):
                tacc[lt, KERNEL] += gains[lt]
            rows = (row_sums(jnp.concatenate(v, axis=0)) for v in (sums1, sums2))
            record(ex2_src, ex2_rcv, block + s, rows)
            activ.append([jnp.concatenate(v, axis=0) for v in acts])
        for peer in tp_peers:
            blocks = pl.ds(block, count)
            remote(ex2_src.at[blocks], ex2_rcv.at[x, blocks], ex2_sem, {"tp": peer}, n).start()
        for s in range(count):
            for lt in range(LT):
                at = pl.ds(pl.multiple_of(first + s * LANES, LANES), LANES)
                act_t[lanes(lt), at] = activ[s][lt].T

    def stage2_big(i, _):
        stage2(i, pl.multiple_of(LANES + i * R, LANES), R)
        return 0

    lax.fori_loop(0, BIG, stage2_big, 0)
    stage2(BIG, *chunks[BIG])
    stage2(BIG + 1, *chunks[BIG + 1])

    cgh = remote(cg_s.at[:, pl.ds(0, HALO), :], cgh_s, cgh_sem, preceding)

    def stage3(n):
        first, size = chunks[n]
        block, count = first // LANES, size // LANES
        for s, total in enumerate(totals(ex2_rcv, ex2_sem, block, count, n)):
            rows = pl.ds(first + s * LANES, LANES)
            mcol[rows, :] = column(total[0:1])
            ncol[rows, :] = column(total[1:2])
        for lt in range(LT):

            def taps_block(j, carry, lt=lt):
                at = pl.multiple_of(first + j * TB, TB)
                rows = pl.ds(at, TB)
                g = rcol[rows, :] * (
                    xg_s[lt, rows, :] - mcol[rows, :] - conv_s[lt, rows, :] * ncol[rows, :]
                )
                cg_s[lt, rows, :] = g
                carry = list(carry)
                for k, window in windows(glu_s, lt, at + 2, TB):
                    carry[k] += folded(g * window)
                return tuple(carry)

            sums = lax.fori_loop(
                0, size // TB, taps_block, tuple(jnp.zeros((8, LANES), F32) for _ in range(KERNEL))
            )
            for k in range(KERNEL):
                tacc[lt, k] += sums[k]

    def back_block(j, _):
        at = pl.multiple_of(j * RB, RB)
        rows = pl.ds(at, RB)
        for lt in range(LT):
            acc = jnp.zeros((RB, LANES), F32)
            for k, window in windows(cg_s, lt, at, RB):
                tap = KERNEL - 1 - k
                acc += taps_s[tap : tap + 1, lanes(lt)] * window
            s = sig_s[lt, rows, :]
            glu = glu_s[lt, pl.ds(pl.multiple_of(at + HALO, RB), RB), :]
            vg_ref[rows, lanes(lt)] = (acc * s).astype(BF16)
            gg_ref[rows, lanes(lt)] = (acc * glu * (1.0 - s)).astype(BF16)
        return 0

    def stage4(first, last):
        lax.fori_loop(first // RB, last // RB, back_block, 0)

    def summed(ref, n):
        total = ref[0].astype(F32)
        for i in range(1, n):
            total += ref[i].astype(F32)
        return total

    D = og_s.shape[1]
    H = D // 2
    Q = H // 2
    B = C // (NZ * NY)
    shape = (C, C)
    i = lax.broadcasted_iota(jnp.int32, shape, 0)
    j = lax.broadcasted_iota(jnp.int32, shape, 1)
    source = ((i // B) % NZ) * (NY * B) + (i // (B * NZ)) * B + i % B
    permutation = jnp.where(j == source, 1.0, 0.0).astype(BF16)
    act_p[...] = jnp.dot(permutation, act_t[...], preferred_element_type=F32).astype(BF16)

    def partial(owner, part):
        columns = pl.ds(pl.multiple_of(owner * H + part * Q, Q), Q)
        rows = (act_t, act_p)[part]
        return jnp.dot(rows[...], og_s[:, columns], preferred_element_type=F32) * FACTOR

    for part in range(2):
        pc_src[part] = partial(1 - c, part).astype(BF16)
    core_copy = remote(pc_src, pc_rcv, pc_sem, partner)
    core_copy.start()
    for part in range(2):
        own_s[part] = partial(c, part)

    stage3(0)

    core_copy.wait()
    N = NZ
    ZB = C // N

    def both_ways(src, dst, sems, swapped):
        z_part, y_part = (1, 0) if swapped else (0, 1)
        for i in z_peers:
            remote(src(z_part, i), dst.at[z_part, z], sems, {"z": i}).start()
        for i in y_peers:
            remote(src(y_part, i), dst.at[y_part, y], sems, {"y": i}).start()

    def finish(dst, sems):
        sample = dst.at[:, pl.ds(0, N - 1)]
        remote(sample, sample, sems, partner).wait()

    for part in range(2):
        own = own_s[part] + pc_rcv[part].astype(F32)
        for i in range(N):
            p1_src[part, i] = own[i * ZB : (i + 1) * ZB].astype(BF16)
    both_ways(lambda part, i: p1_src.at[part, i], p1_rcv, p1_sem, False)
    p1_rcv[0, z] = p1_src[0, z]
    p1_rcv[1, y] = p1_src[1, y]

    for n in range(1, len(chunks)):
        stage3(n)
    cgh.start()

    S = KERNEL + 1
    A = S // 2
    for lt in range(LT):
        tc_src[:, lanes(lt)] = jnp.sum(tacc[lt], axis=1) * FACTOR
    taps_core = remote(tc_src, tc_rcv, tc_sem, partner)
    taps_swap = remote(ts_src, ts_rcv, ts_sem, partner)

    @pl.when(c == 0)
    def _():
        taps_core.start()

    stage4(0, R)

    @pl.when(c == 1)
    def _():
        taps_core.wait_recv()
        both = tc_src[...] + tc_rcv[...]
        t1_src[0] = both[0:A]
        t1_src[1] = both[A:S]
        both_ways(lambda part, i: t1_src.at[part], t1_rcv, t1_sem, False)
        t1_rcv[0, z] = both[0:A]
        t1_rcv[1, y] = both[A:S]

    stage4(R, T - R)
    cgh.wait()
    last = jnp.where(sp == NSP - 1, 0.0, 1.0).astype(F32)
    cg_s[:, pl.ds(T, HALO), :] = cgh_s[...] * last
    stage4(T - R, T)

    finish(p1_rcv, p1_sem)
    for part in range(2):
        sums = summed(p1_rcv.at[part], N)
        for i in range(N):
            p2_src[part, i] = sums[i * B : (i + 1) * B]
    both_ways(lambda part, i: p2_src.at[part, i], p2_rcv, p2_sem, True)
    p2_rcv[0, y] = p2_src[0, y]
    p2_rcv[1, z] = p2_src[1, z]

    @pl.when(c == 1)
    def _():
        finish(t1_rcv, t1_sem)
        half_a, half_b = summed(t1_rcv.at[0], N), summed(t1_rcv.at[1], N)
        t2_src[0] = half_a
        t2_src[1] = half_b
        both_ways(lambda part, i: t2_src.at[part], t2_rcv, t2_sem, True)
        t2_rcv[0, y] = half_a
        t2_rcv[1, z] = half_b

    finish(p2_rcv, p2_sem)
    done_a, done_b = summed(p2_rcv.at[0], N), summed(p2_rcv.at[1], N)
    CB = B // 2
    for i in range(2):
        ps_src[i, :, 0:Q] = done_a[i * CB : (i + 1) * CB]
        ps_src[i, :, Q:H] = done_b[i * CB : (i + 1) * CB]
    proj_swap = remote(ps_src.at[1 - c], ps_rcv, ps_sem, partner)
    proj_swap.start()

    @pl.when(c == 1)
    def _():
        finish(t2_rcv, t2_sem)
        ts_src[0:A] = summed(t2_rcv.at[0], N)
        ts_src[A:S] = summed(t2_rcv.at[1], N)
        taps_swap.start()
        tg_ref[...] = ts_src[0:KERNEL]
        ng_ref[...] = ts_src[KERNEL : KERNEL + 1]

    proj_swap.wait()
    mine, theirs = ps_src[c], ps_rcv[...]
    for i in range(2):
        proj_ref[:, i * H : (i + 1) * H] = jnp.where(c == i, mine, theirs)
    halo.wait_send()
    for rcv, sem in ((ex1_rcv, ex1_sem), (ex2_rcv, ex2_sem)):
        sample = rcv.at[pl.ds(0, NTP - 1)]
        remote(sample, sample, sem, partner).wait_send()

    @pl.when(c == 1)
    def _():
        taps_swap.wait_send()

    @pl.when(c == 0)
    def _():
        taps_core.wait_send()
        taps_swap.wait_recv()
        tg_ref[...] = ts_rcv[0:KERNEL]
        ng_ref[...] = ts_rcv[KERNEL : KERNEL + 1]


def store_kernel(*refs):
    n = len(refs) // 2
    sems = refs[-1]
    copies = [pltpu.make_async_copy(refs[i], refs[n + i], sems.at[i]) for i in range(n)]
    for copy in copies:
        copy.start()
    for copy in copies:
        copy.wait()


def per_device(sizes, glu_value, glu_gate, conv_taps, channel_gain, proj_weight, out_grad):
    NZ, NY, NTP = sizes
    T, C = glu_value.shape
    K = conv_taps.shape[0]
    D = out_grad.shape[1]
    LT, S, A = C // LANES, K + 1, (K + 1) // 2
    N, ZB, B = NZ, C // NZ, C // (NZ * NY)
    NBLK = T // LANES
    NCH = (T - 2 * LANES) // R + 2
    CB = B // 2
    H, Q = D // 2, D // 4
    factor = float(1.0 / (T * NZ * NY * 2) ** 0.5)
    params = (NZ, NY, NTP, T, C, K, C * NTP, factor)
    full = (LT, T, LANES)
    vmem, dma = pltpu.VMEM, pltpu.SemaphoreType.DMA
    any_spec = pl.BlockSpec(memory_space=pltpu.HBM)
    vmem_spec = pl.BlockSpec(memory_space=pltpu.VMEM)
    scratch = [
        vmem((T, C), BF16), vmem((T, C), BF16), vmem((K, C), F32), vmem((1, C), F32),
        vmem((C, D), BF16), vmem((T, D), BF16),
        vmem((2, HALO, C), BF16),
        vmem((LT, T + HALO, LANES), F32), vmem(full, F32), vmem(full, F32), vmem(full, F32), vmem(full, F32),
        vmem((C, T), BF16), vmem((C, T), BF16),
        vmem((T, LANES), F32), vmem((T, LANES), F32), vmem((T, LANES), F32),
        vmem((LT, T + HALO, LANES), F32), vmem((LT, HALO, LANES), F32),
        vmem((LT, S, 8, LANES), F32),
        vmem((NBLK, 2, LANES), F32), vmem((NTP, NBLK, 2, LANES), F32),
        vmem((NBLK, 2, LANES), F32), vmem((NTP, NBLK, 2, LANES), F32),
        vmem((2, C, Q), BF16), vmem((2, C, Q), BF16), vmem((2, C, Q), F32),
        vmem((2, N, ZB, Q), BF16), vmem((2, N, ZB, Q), BF16),
        vmem((2, N, B, Q), F32), vmem((2, N, B, Q), F32),
        vmem((2, CB, H), F32), vmem((CB, H), F32),
        vmem((S, C), F32), vmem((S, C), F32),
        vmem((2, A, C), F32), vmem((2, N, A, C), F32),
        vmem((2, A, C), F32), vmem((2, N, A, C), F32),
        vmem((S, C), F32), vmem((S, C), F32),
        dma((6,)), dma((2,)), dma((1 + NCH,)), dma((1 + NCH,)), dma((2,)),
    ] + [dma((2,))] * 8 + [
    ]
    results = (
        jax.ShapeDtypeStruct((T, C), BF16),
        jax.ShapeDtypeStruct((T, C), BF16),
        jax.ShapeDtypeStruct((CB, D), F32),
        jax.ShapeDtypeStruct((K, C), F32),
        jax.ShapeDtypeStruct((1, C), F32),
    )
    held = pl.pallas_call(
        functools.partial(kernel, params),
        out_shape=results,
        in_specs=[any_spec] * 6,
        out_specs=(vmem_spec,) * 5,
        scratch_shapes=scratch,
        compiler_params=pltpu.CompilerParams(
            collective_id=0, has_side_effects=True, vmem_limit_bytes=40 * 2**20
        ),
    )(*(
        pltpu.with_memory_space_constraint(a, pltpu.HBM)
        for a in (glu_value, glu_gate, conv_taps, channel_gain[None], proj_weight, out_grad)
    ))
    value_grad, gate_grad, proj_grad, taps_grad, gain_grad = pl.pallas_call(
        store_kernel,
        out_shape=results,
        in_specs=[vmem_spec] * 5,
        out_specs=(any_spec,) * 5,
        scratch_shapes=[dma((5,))],
        compiler_params=pltpu.CompilerParams(vmem_limit_bytes=8 * 2**20),
    )(*held)
    return value_grad, gate_grad, proj_grad, taps_grad, gain_grad[0]


def solution(mesh):
    return sized(mesh, 8, 8)


def sized(mesh, nz, ny):
    tp = mesh.shape["tp"]
    finer = Mesh(mesh.devices.reshape(nz, ny, 2, tp), ("z", "y", "c", "tp"))
    return jax.shard_map(
        functools.partial(per_device, (nz, ny, tp)),
        mesh=finer,
        in_specs=(P(SP, "tp"), P(SP, "tp"), P(None, "tp"), P("tp"), P("tp", None), P(SP, None)),
        out_specs=(P(SP, "tp"), P(SP, "tp"), P(TP_SP, None), P(None, "tp"), P("tp")),
        check_vma=False,
    )
```

```python
import functools

import jax
import jax.numpy as jnp
from jax import lax
from jax.experimental import pallas as pl
from jax.experimental.pallas import tpu as pltpu
from jax.sharding import Mesh
from jax.sharding import PartitionSpec as P

MESH = pl.DeviceIdType.MESH
SP = ("z", "y", "c")
TP_SP = ("tp", "z", "y", "c")
F32, BF16 = jnp.float32, jnp.bfloat16
HALO = 32
LANES = 128
R = 256
RB = 32
GB = 64
VB = 64
NB = 32
TB = 64
AB = 512


def sigmoid(x):
    return 0.5 * jnp.tanh(0.5 * x) + 0.5


def folded(x):
    return jnp.sum(x.reshape(-1, 8, x.shape[-1]), axis=0)


def kernel(
    sizes,
    value_hbm, gate_hbm, taps_hbm, gain_hbm, w_hbm, og_hbm,
    vg_ref, gg_ref, proj_ref, tg_ref, ng_ref,
    value_s, gate_s, taps_s, gain_s, w_s, og_s,
    hv_s, glu_s, sig_s, conv_s, xg_s, ag_s, act_t, act_p,
    rcol, mcol, ncol, cg_s, cgh_s, tacc,
    ex1_src, ex1_rcv, ex2_src, ex2_rcv,
    pc_src, pc_rcv, own_s, p1_src, p1_rcv, p2_src, p2_rcv, ps_src, ps_rcv,
    tc_src, tc_rcv, t1_src, t1_rcv, t2_src, t2_rcv, ts_src, ts_rcv,
    lsem, hsem, ex1_sem, ex2_sem, cgh_sem, pc_sem, p1_sem, p2_sem, ps_sem, tc_sem, t1_sem, t2_sem, ts_sem, rounds,
):
    NZ, NY, NTP, T, C, KERNEL, CH, FACTOR = sizes
    NBLK = T // LANES
    BIG = (T - 2 * LANES) // R
    chunks = [(LANES + i * R, R) for i in range(BIG)] + [(T - LANES, LANES), (0, LANES)]
    LT = C // LANES
    z, y, c, x = (lax.axis_index(a) for a in ("z", "y", "c", "tp"))
    sp = (z * NY + y) * 2 + c
    NSP = NZ * NY * 2
    partner = {"c": 1 - c}

    def at_sp(i):
        return {"z": i // (NY * 2), "y": lax.rem(i // 2, NY), "c": lax.rem(i, 2)}

    following, preceding = at_sp(lax.rem(sp + 1, NSP)), at_sp(lax.rem(sp + NSP - 1, NSP))

    def others(i, n):
        return [lax.rem(i + d, n) for d in sorted(range(1, n), key=lambda d: -min(d, n - d))]

    tp_peers, y_peers, z_peers = others(x, NTP), others(y, NY), others(z, NZ)

    def remote(src, dst, sems, device, i=0):
        return pltpu.make_async_remote_copy(
            src_ref=src, dst_ref=dst, send_sem=sems.at[0], recv_sem=sems.at[1 + i],
            device_id=device, device_id_type=MESH,
        )

    barrier = pltpu.get_barrier_semaphore()
    near = [{"y": lax.rem(y + d, NY)} for d in (1, NY - 1)] + [{"z": lax.rem(z + d, NZ)} for d in (1, NZ - 1)]
    peers = [partner, following, preceding] + [{"tp": i} for i in tp_peers] + near

    ROUNDS = NY // 2 - 1

    def tell(r):
        for device in near:
            pl.semaphore_signal(rounds.at[r], inc=1, device_id=device, device_id_type=MESH)

    def hear(r):
        pl.semaphore_wait(rounds.at[r], len(near))
        if r + 1 < ROUNDS:
            tell(r + 1)


    loads = [
        pltpu.make_async_copy(src, dst, lsem.at[i])
        for i, (src, dst) in enumerate(
            ((value_hbm, value_s), (gate_hbm, gate_s), (taps_hbm, taps_s), (gain_hbm, gain_s), (w_hbm, w_s), (og_hbm, og_s))
        )
    ]
    for copy in loads:
        copy.start()
    for device in peers:
        pl.semaphore_signal(barrier, inc=1, device_id=device, device_id_type=MESH)

    loads[0].wait()
    loads[1].wait()

    def lanes(lt):
        return slice(lt * LANES, (lt + 1) * LANES)

    def glu_block(i, _):
        rows = pl.ds(pl.multiple_of(i * GB, GB), GB)
        into = pl.ds(pl.multiple_of(HALO + i * GB, HALO), GB)
        for lt in range(LT):
            s = sigmoid(gate_s[rows, lanes(lt)].astype(F32))
            sig_s[lt, rows, :] = s
            glu_s[lt, into, :] = value_s[rows, lanes(lt)].astype(F32) * s
        return 0

    lax.fori_loop(0, T // GB, glu_block, 0)

    pl.semaphore_wait(barrier, len(peers))
    tell(0)
    tail = pl.ds(T - HALO, HALO)
    remote(value_s.at[tail], hv_s.at[0], hsem, following).start()
    remote(gate_s.at[tail], hv_s.at[1], hsem, following).start()
    halo = remote(hv_s, hv_s, hsem, following)
    tacc[...] = jnp.zeros_like(tacc)
    loads[2].wait()
    loads[3].wait()

    def exchange(src, rcv, sem, n):
        first, size = chunks[n]
        blocks = pl.ds(first // LANES, size // LANES)
        for peer in tp_peers:
            remote(src.at[blocks], rcv.at[x, blocks], sem, {"tp": peer}, n).start()

    def received(rcv, sem, block, count, n):
        sample = rcv.at[pl.ds(0, NTP - 1), pl.ds(block, count)]
        remote(sample, sample, sem, partner, n).wait_recv()

    def record(src, rcv, block, rows):
        for i, row in enumerate(rows):
            src[block, i : i + 1, :] = row
            rcv[x, block, i : i + 1, :] = row

    def row_sums(v):
        return jnp.sum(v.T, axis=0, keepdims=True)

    def windows(ref, lt, at, size):
        for s in range(8):
            steps = len(range(s, KERNEL, 8))
            wide = ref[lt, pl.ds(at + s, size + 8 * (steps - 1)), :]
            for m in range(steps):
                yield s + 8 * m, wide[8 * m : 8 * m + size]

    def conv_stats(block):
        rows = pl.ds(pl.multiple_of(block * LANES, LANES), LANES)
        total, square = 0.0, 0.0
        for lt in range(LT):
            v = conv_s[lt, rows, :]
            total, square = total + v, square + v * v
        return row_sums(total), row_sums(square)

    def conv_block(block):
        for lt in range(LT):
            for half in range(LANES // VB):
                at = pl.multiple_of(block * LANES + half * VB, VB)
                acc = jnp.zeros((VB, LANES), F32)
                for k, window in windows(glu_s, lt, at + 2, VB):
                    acc += taps_s[k : k + 1, lanes(lt)] * window
                conv_s[lt, pl.ds(at, VB), :] = acc

    conv_block(1)

    def stage1(block, _):
        sums = conv_stats(block)

        conv_block(lax.rem(block + 1, NBLK))
        record(ex1_src, ex1_rcv, block, sums)
        for n, (first, size) in enumerate(chunks[:-1]):

            @pl.when(block == (first + size) // LANES - 1)
            def _(n=n):
                exchange(ex1_src, ex1_rcv, ex1_sem, n)

        @pl.when(block == NBLK - 2)
        def _():
            halo.wait_recv()
            keep = jnp.where(sp == 0, 0.0, 1.0).astype(F32)
            for lt in range(LT):
                s = sigmoid(hv_s[1, :, lanes(lt)].astype(F32)) * keep
                glu_s[lt, pl.ds(0, HALO), :] = hv_s[0, :, lanes(lt)].astype(F32) * s

        return 0

    lax.fori_loop(1, NBLK, stage1, 0)
    record(ex1_src, ex1_rcv, 0, conv_stats(0))
    exchange(ex1_src, ex1_rcv, ex1_sem, len(chunks) - 1)

    hear(0)
    loads[4].wait()
    loads[5].wait()

    def act_grad_block(i, _):
        rows = pl.ds(pl.multiple_of(i * AB, AB), AB)
        g = lax.dot_general(
            og_s[rows, :], w_s[...], (((1,), (1,)), ((), ())), preferred_element_type=F32
        )
        for lt in range(LT):
            ag_s[lt, rows, :] = g[:, lanes(lt)]
        return 0

    lax.fori_loop(0, T // AB, act_grad_block, 0)

    hear(1)

    def column(row):
        return jnp.broadcast_to(row, (LANES, LANES)).T

    def totals(rcv, sem, block, count, n):
        received(rcv, sem, block, count, n)
        both = []
        for s in range(count):
            total = rcv[0, block + s]
            for t in range(1, NTP):
                total += rcv[t, block + s]
            both.append(total * (1.0 / CH))
        return both

    def stage2(n, first, size):
        block, count = first // LANES, size // LANES
        activ = []
        for s, total in enumerate(totals(ex1_rcv, ex1_sem, block, count, n)):
            mean = total[0:1]
            inv = lax.rsqrt(total[1:2] - mean * mean + 1e-05)
            m, r = column(mean), column(inv)
            start = first + s * LANES
            rcol[pl.ds(pl.multiple_of(start, LANES), LANES), :] = r
            sums1, sums2, acts = [], [], [[] for _ in range(LT)]
            gains = [0.0] * LT
            for j in range(0, LANES, NB):
                rows = pl.ds(pl.multiple_of(start + j, NB), NB)
                s1, s2 = 0.0, 0.0
                for lt in range(LT):
                    gain = gain_s[0:1, lanes(lt)]
                    xhat = (conv_s[lt, rows, :] - m[j : j + NB]) * r[j : j + NB]
                    n_ = xhat * gain
                    g = sigmoid(n_)
                    acts[lt].append((n_ * g).astype(BF16))
                    ng = ag_s[lt, rows, :] * (g * (1.0 + n_ * (1.0 - g)))
                    xg = ng * gain
                    conv_s[lt, rows, :] = xhat
                    xg_s[lt, rows, :] = xg
                    s1, s2 = s1 + xg, s2 + xg * xhat
                    gains[lt] += folded(ng * xhat)
                sums1.append(s1)
                sums2.append(s2)
            for lt in range(LT):
                tacc[lt, KERNEL] += gains[lt]
            rows = (row_sums(jnp.concatenate(v, axis=0)) for v in (sums1, sums2))
            record(ex2_src, ex2_rcv, block + s, rows)
            activ.append([jnp.concatenate(v, axis=0) for v in acts])
        for peer in tp_peers:
            blocks = pl.ds(block, count)
            remote(ex2_src.at[blocks], ex2_rcv.at[x, blocks], ex2_sem, {"tp": peer}, n).start()
        for s in range(count):
            for lt in range(LT):
                at = pl.ds(pl.multiple_of(first + s * LANES, LANES), LANES)
                act_t[lanes(lt), at] = activ[s][lt].T

    def stage2_big(i, _):
        stage2(i, pl.multiple_of(LANES + i * R, LANES), R)
        return 0

    lax.fori_loop(0, BIG, stage2_big, 0)
    stage2(BIG, *chunks[BIG])
    stage2(BIG + 1, *chunks[BIG + 1])

    cgh = remote(cg_s.at[:, pl.ds(0, HALO), :], cgh_s, cgh_sem, preceding)

    def stage3(n):
        first, size = chunks[n]
        block, count = first // LANES, size // LANES
        for s, total in enumerate(totals(ex2_rcv, ex2_sem, block, count, n)):
            rows = pl.ds(first + s * LANES, LANES)
            mcol[rows, :] = column(total[0:1])
            ncol[rows, :] = column(total[1:2])
        for lt in range(LT):

            def taps_block(j, carry, lt=lt):
                at = pl.multiple_of(first + j * TB, TB)
                rows = pl.ds(at, TB)
                g = rcol[rows, :] * (
                    xg_s[lt, rows, :] - mcol[rows, :] - conv_s[lt, rows, :] * ncol[rows, :]
                )
                cg_s[lt, rows, :] = g
                carry = list(carry)
                for k, window in windows(glu_s, lt, at + 2, TB):
                    carry[k] += folded(g * window)
                return tuple(carry)

            sums = lax.fori_loop(
                0, size // TB, taps_block, tuple(jnp.zeros((8, LANES), F32) for _ in range(KERNEL))
            )
            for k in range(KERNEL):
                tacc[lt, k] += sums[k]

    def back_block(j, _):
        at = pl.multiple_of(j * RB, RB)
        rows = pl.ds(at, RB)
        for lt in range(LT):
            acc = jnp.zeros((RB, LANES), F32)
            for k, window in windows(cg_s, lt, at, RB):
                tap = KERNEL - 1 - k
                acc += taps_s[tap : tap + 1, lanes(lt)] * window
            s = sig_s[lt, rows, :]
            glu = glu_s[lt, pl.ds(pl.multiple_of(at + HALO, RB), RB), :]
            vg_ref[rows, lanes(lt)] = (acc * s).astype(BF16)
            gg_ref[rows, lanes(lt)] = (acc * glu * (1.0 - s)).astype(BF16)
        return 0

    def stage4(first, last):
        lax.fori_loop(first // RB, last // RB, back_block, 0)

    def summed(ref, n):
        total = ref[0].astype(F32)
        for i in range(1, n):
            total += ref[i].astype(F32)
        return total

    D = og_s.shape[1]
    H = D // 2
    Q = H // 2
    B = C // (NZ * NY)
    shape = (C, C)
    i = lax.broadcasted_iota(jnp.int32, shape, 0)
    j = lax.broadcasted_iota(jnp.int32, shape, 1)
    source = ((i // B) % NZ) * (NY * B) + (i // (B * NZ)) * B + i % B
    permutation = jnp.where(j == source, 1.0, 0.0).astype(BF16)
    act_p[...] = jnp.dot(permutation, act_t[...], preferred_element_type=F32).astype(BF16)

    def partial(owner, part):
        columns = pl.ds(pl.multiple_of(owner * H + part * Q, Q), Q)
        rows = (act_t, act_p)[part]
        return jnp.dot(rows[...], og_s[:, columns], preferred_element_type=F32) * FACTOR

    for part in range(2):
        pc_src[part] = partial(1 - c, part).astype(BF16)
    core_copy = remote(pc_src, pc_rcv, pc_sem, partner)
    core_copy.start()
    hear(2)
    for part in range(2):
        own_s[part] = partial(c, part)

    stage3(0)

    core_copy.wait()
    N = NZ
    ZB = C // N

    def both_ways(src, dst, sems, swapped):
        z_part, y_part = (1, 0) if swapped else (0, 1)
        for i in z_peers:
            remote(src(z_part, i), dst.at[z_part, z], sems, {"z": i}).start()
        for i in y_peers:
            remote(src(y_part, i), dst.at[y_part, y], sems, {"y": i}).start()

    def finish(dst, sems):
        sample = dst.at[:, pl.ds(0, N - 1)]
        remote(sample, sample, sems, partner).wait()

    for part in range(2):
        own = own_s[part] + pc_rcv[part].astype(F32)
        for i in range(N):
            p1_src[part, i] = own[i * ZB : (i + 1) * ZB].astype(BF16)
    both_ways(lambda part, i: p1_src.at[part, i], p1_rcv, p1_sem, False)
    p1_rcv[0, z] = p1_src[0, z]
    p1_rcv[1, y] = p1_src[1, y]

    for n in range(1, len(chunks)):
        stage3(n)
    cgh.start()

    S = KERNEL + 1
    A = S // 2
    for lt in range(LT):
        tc_src[:, lanes(lt)] = jnp.sum(tacc[lt], axis=1) * FACTOR
    taps_core = remote(tc_src, tc_rcv, tc_sem, partner)
    taps_swap = remote(ts_src, ts_rcv, ts_sem, partner)

    @pl.when(c == 0)
    def _():
        taps_core.start()

    stage4(0, R)

    @pl.when(c == 1)
    def _():
        taps_core.wait_recv()
        both = tc_src[...] + tc_rcv[...]
        t1_src[0] = both[0:A]
        t1_src[1] = both[A:S]
        both_ways(lambda part, i: t1_src.at[part], t1_rcv, t1_sem, False)
        t1_rcv[0, z] = both[0:A]
        t1_rcv[1, y] = both[A:S]

    stage4(R, T - R)
    cgh.wait()
    last = jnp.where(sp == NSP - 1, 0.0, 1.0).astype(F32)
    cg_s[:, pl.ds(T, HALO), :] = cgh_s[...] * last
    stage4(T - R, T)

    finish(p1_rcv, p1_sem)
    for part in range(2):
        sums = summed(p1_rcv.at[part], N)
        for i in range(N):
            p2_src[part, i] = sums[i * B : (i + 1) * B]
    both_ways(lambda part, i: p2_src.at[part, i], p2_rcv, p2_sem, True)
    p2_rcv[0, y] = p2_src[0, y]
    p2_rcv[1, z] = p2_src[1, z]

    @pl.when(c == 1)
    def _():
        finish(t1_rcv, t1_sem)
        half_a, half_b = summed(t1_rcv.at[0], N), summed(t1_rcv.at[1], N)
        t2_src[0] = half_a
        t2_src[1] = half_b
        both_ways(lambda part, i: t2_src.at[part], t2_rcv, t2_sem, True)
        t2_rcv[0, y] = half_a
        t2_rcv[1, z] = half_b

    finish(p2_rcv, p2_sem)
    done_a, done_b = summed(p2_rcv.at[0], N), summed(p2_rcv.at[1], N)
    CB = B // 2
    for i in range(2):
        ps_src[i, :, 0:Q] = done_a[i * CB : (i + 1) * CB]
        ps_src[i, :, Q:H] = done_b[i * CB : (i + 1) * CB]
    proj_swap = remote(ps_src.at[1 - c], ps_rcv, ps_sem, partner)
    proj_swap.start()

    @pl.when(c == 1)
    def _():
        finish(t2_rcv, t2_sem)
        ts_src[0:A] = summed(t2_rcv.at[0], N)
        ts_src[A:S] = summed(t2_rcv.at[1], N)
        taps_swap.start()
        tg_ref[...] = ts_src[0:KERNEL]
        ng_ref[...] = ts_src[KERNEL : KERNEL + 1]

    proj_swap.wait()
    mine, theirs = ps_src[c], ps_rcv[...]
    for i in range(2):
        proj_ref[:, i * H : (i + 1) * H] = jnp.where(c == i, mine, theirs)
    halo.wait_send()
    for rcv, sem in ((ex1_rcv, ex1_sem), (ex2_rcv, ex2_sem)):
        sample = rcv.at[pl.ds(0, NTP - 1)]
        remote(sample, sample, sem, partner).wait_send()

    @pl.when(c == 1)
    def _():
        taps_swap.wait_send()

    @pl.when(c == 0)
    def _():
        taps_core.wait_send()
        taps_swap.wait_recv()
        tg_ref[...] = ts_rcv[0:KERNEL]
        ng_ref[...] = ts_rcv[KERNEL : KERNEL + 1]


def store_kernel(*refs):
    n = len(refs) // 2
    sems = refs[-1]
    copies = [pltpu.make_async_copy(refs[i], refs[n + i], sems.at[i]) for i in range(n)]
    for copy in copies:
        copy.start()
    for copy in copies:
        copy.wait()


def per_device(sizes, glu_value, glu_gate, conv_taps, channel_gain, proj_weight, out_grad):
    NZ, NY, NTP = sizes
    T, C = glu_value.shape
    K = conv_taps.shape[0]
    D = out_grad.shape[1]
    LT, S, A = C // LANES, K + 1, (K + 1) // 2
    N, ZB, B = NZ, C // NZ, C // (NZ * NY)
    NBLK = T // LANES
    NCH = (T - 2 * LANES) // R + 2
    CB = B // 2
    H, Q = D // 2, D // 4
    factor = float(1.0 / (T * NZ * NY * 2) ** 0.5)
    params = (NZ, NY, NTP, T, C, K, C * NTP, factor)
    full = (LT, T, LANES)
    vmem, dma = pltpu.VMEM, pltpu.SemaphoreType.DMA
    any_spec = pl.BlockSpec(memory_space=pltpu.HBM)
    vmem_spec = pl.BlockSpec(memory_space=pltpu.VMEM)
    scratch = [
        vmem((T, C), BF16), vmem((T, C), BF16), vmem((K, C), F32), vmem((1, C), F32),
        vmem((C, D), BF16), vmem((T, D), BF16),
        vmem((2, HALO, C), BF16),
        vmem((LT, T + HALO, LANES), F32), vmem(full, F32), vmem(full, F32), vmem(full, F32), vmem(full, F32),
        vmem((C, T), BF16), vmem((C, T), BF16),
        vmem((T, LANES), F32), vmem((T, LANES), F32), vmem((T, LANES), F32),
        vmem((LT, T + HALO, LANES), F32), vmem((LT, HALO, LANES), F32),
        vmem((LT, S, 8, LANES), F32),
        vmem((NBLK, 2, LANES), F32), vmem((NTP, NBLK, 2, LANES), F32),
        vmem((NBLK, 2, LANES), F32), vmem((NTP, NBLK, 2, LANES), F32),
        vmem((2, C, Q), BF16), vmem((2, C, Q), BF16), vmem((2, C, Q), F32),
        vmem((2, N, ZB, Q), BF16), vmem((2, N, ZB, Q), BF16),
        vmem((2, N, B, Q), F32), vmem((2, N, B, Q), F32),
        vmem((2, CB, H), F32), vmem((CB, H), F32),
        vmem((S, C), F32), vmem((S, C), F32),
        vmem((2, A, C), F32), vmem((2, N, A, C), F32),
        vmem((2, A, C), F32), vmem((2, N, A, C), F32),
        vmem((S, C), F32), vmem((S, C), F32),
        dma((6,)), dma((2,)), dma((1 + NCH,)), dma((1 + NCH,)), dma((2,)),
    ] + [dma((2,))] * 8 + [pltpu.SemaphoreType.REGULAR((max(NY // 2 - 1, 1),))]
    results = (
        jax.ShapeDtypeStruct((T, C), BF16),
        jax.ShapeDtypeStruct((T, C), BF16),
        jax.ShapeDtypeStruct((CB, D), F32),
        jax.ShapeDtypeStruct((K, C), F32),
        jax.ShapeDtypeStruct((1, C), F32),
    )
    held = pl.pallas_call(
        functools.partial(kernel, params),
        out_shape=results,
        in_specs=[any_spec] * 6,
        out_specs=(vmem_spec,) * 5,
        scratch_shapes=scratch,
        compiler_params=pltpu.CompilerParams(
            collective_id=0, has_side_effects=True, vmem_limit_bytes=40 * 2**20
        ),
    )(*(
        pltpu.with_memory_space_constraint(a, pltpu.HBM)
        for a in (glu_value, glu_gate, conv_taps, channel_gain[None], proj_weight, out_grad)
    ))
    value_grad, gate_grad, proj_grad, taps_grad, gain_grad = pl.pallas_call(
        store_kernel,
        out_shape=results,
        in_specs=[vmem_spec] * 5,
        out_specs=(any_spec,) * 5,
        scratch_shapes=[dma((5,))],
        compiler_params=pltpu.CompilerParams(vmem_limit_bytes=8 * 2**20),
    )(*held)
    return value_grad, gate_grad, proj_grad, taps_grad, gain_grad[0]


def solution(mesh):
    return sized(mesh, 8, 8)


def sized(mesh, nz, ny):
    tp = mesh.shape["tp"]
    finer = Mesh(mesh.devices.reshape(nz, ny, 2, tp), ("z", "y", "c", "tp"))
    return jax.shard_map(
        functools.partial(per_device, (nz, ny, tp)),
        mesh=finer,
        in_specs=(P(SP, "tp"), P(SP, "tp"), P(None, "tp"), P("tp"), P("tp", None), P(SP, None)),
        out_specs=(P(SP, "tp"), P(SP, "tp"), P(TP_SP, None), P(None, "tp"), P("tp")),
        check_vma=False,
    )
```

```python
import functools

import jax
import jax.numpy as jnp
from jax import lax
from jax.experimental import pallas as pl
from jax.experimental.pallas import tpu as pltpu
from jax.sharding import Mesh
from jax.sharding import PartitionSpec as P

MESH = pl.DeviceIdType.MESH
SP = ("z", "y", "c")
TP_SP = ("tp", "z", "y", "c")
F32, BF16 = jnp.float32, jnp.bfloat16
HALO = 32
LANES = 128
R = 256
RB = 32
GB = 64
VB = 64
NB = 32
TB = 64
AB = 512


def sigmoid(x):
    return 0.5 * jnp.tanh(0.5 * x) + 0.5


def folded(x):
    return jnp.sum(x.reshape(-1, 8, x.shape[-1]), axis=0)


def kernel(
    sizes,
    value_hbm, gate_hbm, taps_hbm, gain_hbm, w_hbm, og_hbm,
    vg_ref, gg_ref, proj_ref, tg_ref, ng_ref,
    value_s, gate_s, taps_s, gain_s, w_s, og_s,
    hv_s, glu_s, sig_s, conv_s, xg_s, ag_s, act_t, act_p,
    rcol, mcol, ncol, cg_s, cgh_s, tacc,
    ex1_src, ex1_rcv, ex2_src, ex2_rcv,
    pc_src, pc_rcv, own_s, p1_src, p1_rcv, p2_src, p2_rcv, ps_src, ps_rcv,
    tc_src, tc_rcv, t1_src, t1_rcv, t2_src, t2_rcv, ts_src, ts_rcv,
    lsem, hsem, ex1_sem, ex2_sem, cgh_sem, pc_sem, p1_sem, p2_sem, ps_sem, tc_sem, t1_sem, t2_sem, ts_sem, rounds,
):
    NZ, NY, NTP, T, C, KERNEL, CH, FACTOR = sizes
    NBLK = T // LANES
    BIG = (T - 2 * LANES) // R
    chunks = [(LANES + i * R, R) for i in range(BIG)] + [(T - LANES, LANES), (0, LANES)]
    LT = C // LANES
    z, y, c, x = (lax.axis_index(a) for a in ("z", "y", "c", "tp"))
    sp = (z * NY + y) * 2 + c
    NSP = NZ * NY * 2
    partner = {"c": 1 - c}

    def at_sp(i):
        return {"z": i // (NY * 2), "y": lax.rem(i // 2, NY), "c": lax.rem(i, 2)}

    following, preceding = at_sp(lax.rem(sp + 1, NSP)), at_sp(lax.rem(sp + NSP - 1, NSP))

    def others(i, n):
        return [lax.rem(i + d, n) for d in sorted(range(1, n), key=lambda d: -min(d, n - d))]

    tp_peers, y_peers, z_peers = others(x, NTP), others(y, NY), others(z, NZ)

    def remote(src, dst, sems, device, i=0):
        return pltpu.make_async_remote_copy(
            src_ref=src, dst_ref=dst, send_sem=sems.at[0], recv_sem=sems.at[1 + i],
            device_id=device, device_id_type=MESH,
        )

    barrier = pltpu.get_barrier_semaphore()
    near = [{"y": lax.rem(y + d, NY)} for d in (1, NY - 1)] + [{"z": lax.rem(z + d, NZ)} for d in (1, NZ - 1)]
    peers = [partner, following, preceding] + [{"tp": i} for i in tp_peers] + near

    ROUNDS = NY // 2 - 1

    def tell(r):
        for device in near:
            pl.semaphore_signal(rounds.at[r], inc=1, device_id=device, device_id_type=MESH)

    def hear(r):
        pl.semaphore_wait(rounds.at[r], len(near))
        if r + 1 < ROUNDS:
            tell(r + 1)


    loads = [
        pltpu.make_async_copy(src, dst, lsem.at[i])
        for i, (src, dst) in enumerate(
            ((value_hbm, value_s), (gate_hbm, gate_s), (taps_hbm, taps_s), (gain_hbm, gain_s), (w_hbm, w_s), (og_hbm, og_s))
        )
    ]
    for copy in loads:
        copy.start()
    for device in peers:
        pl.semaphore_signal(barrier, inc=1, device_id=device, device_id_type=MESH)

    loads[0].wait()
    loads[1].wait()

    def lanes(lt):
        return slice(lt * LANES, (lt + 1) * LANES)

    def glu_block(i, _):
        rows = pl.ds(pl.multiple_of(i * GB, GB), GB)
        into = pl.ds(pl.multiple_of(HALO + i * GB, HALO), GB)
        for lt in range(LT):
            s = sigmoid(gate_s[rows, lanes(lt)].astype(F32))
            sig_s[lt, rows, :] = s
            glu_s[lt, into, :] = value_s[rows, lanes(lt)].astype(F32) * s
        return 0

    lax.fori_loop(0, T // GB, glu_block, 0)

    pl.semaphore_wait(barrier, len(peers))
    tell(0)
    tail = pl.ds(T - HALO, HALO)
    remote(value_s.at[tail], hv_s.at[0], hsem, following).start()
    remote(gate_s.at[tail], hv_s.at[1], hsem, following).start()
    halo = remote(hv_s, hv_s, hsem, following)
    tacc[...] = jnp.zeros_like(tacc)
    loads[2].wait()
    loads[3].wait()

    def exchange(src, rcv, sem, n):
        first, size = chunks[n]
        blocks = pl.ds(first // LANES, size // LANES)
        for peer in tp_peers:
            remote(src.at[blocks], rcv.at[x, blocks], sem, {"tp": peer}, n).start()

    def received(rcv, sem, block, count, n):
        sample = rcv.at[pl.ds(0, NTP - 1), pl.ds(block, count)]
        remote(sample, sample, sem, partner, n).wait_recv()

    def record(src, rcv, block, rows):
        for i, row in enumerate(rows):
            src[block, i : i + 1, :] = row
            rcv[x, block, i : i + 1, :] = row

    def row_sums(v):
        return jnp.sum(v.T, axis=0, keepdims=True)

    def windows(ref, lt, at, size):
        for s in range(8):
            steps = len(range(s, KERNEL, 8))
            wide = ref[lt, pl.ds(at + s, size + 8 * (steps - 1)), :]
            for m in range(steps):
                yield s + 8 * m, wide[8 * m : 8 * m + size]

    def conv_stats(block):
        rows = pl.ds(pl.multiple_of(block * LANES, LANES), LANES)
        total, square = 0.0, 0.0
        for lt in range(LT):
            v = conv_s[lt, rows, :]
            total, square = total + v, square + v * v
        return row_sums(total), row_sums(square)

    def conv_block(block, halves=range(LANES // VB)):
        for lt in range(LT):
            for half in halves:
                at = pl.multiple_of(block * LANES + half * VB, VB)
                acc = jnp.zeros((VB, LANES), F32)
                for k, window in windows(glu_s, lt, at + 2, VB):
                    acc += taps_s[k : k + 1, lanes(lt)] * window
                conv_s[lt, pl.ds(at, VB), :] = acc

    conv_block(1)

    def stage1(block, _):
        sums = conv_stats(block)

        conv_block(block + 1)
        record(ex1_src, ex1_rcv, block, sums)
        for n, (first, size) in enumerate(chunks[:-2]):

            @pl.when(block == (first + size) // LANES - 1)
            def _(n=n):
                exchange(ex1_src, ex1_rcv, ex1_sem, n)

        return 0

    lax.fori_loop(1, NBLK - 1, stage1, 0)

    sums = conv_stats(NBLK - 1)
    conv_block(0, range(1, LANES // VB))
    record(ex1_src, ex1_rcv, NBLK - 1, sums)
    exchange(ex1_src, ex1_rcv, ex1_sem, len(chunks) - 2)
    halo.wait_recv()
    keep = jnp.where(sp == 0, 0.0, 1.0).astype(F32)
    for lt in range(LT):
        s = sigmoid(hv_s[1, :, lanes(lt)].astype(F32)) * keep
        glu_s[lt, pl.ds(0, HALO), :] = hv_s[0, :, lanes(lt)].astype(F32) * s
    conv_block(0, range(1))
    record(ex1_src, ex1_rcv, 0, conv_stats(0))
    exchange(ex1_src, ex1_rcv, ex1_sem, len(chunks) - 1)

    hear(0)
    loads[4].wait()
    loads[5].wait()

    def act_grad_block(i, _):
        rows = pl.ds(pl.multiple_of(i * AB, AB), AB)
        g = lax.dot_general(
            og_s[rows, :], w_s[...], (((1,), (1,)), ((), ())), preferred_element_type=F32
        )
        for lt in range(LT):
            ag_s[lt, rows, :] = g[:, lanes(lt)]
        return 0

    lax.fori_loop(0, T // AB, act_grad_block, 0)

    hear(1)

    def column(row):
        return jnp.broadcast_to(row, (LANES, LANES)).T

    def totals(rcv, sem, block, count, n):
        received(rcv, sem, block, count, n)
        both = []
        for s in range(count):
            total = rcv[0, block + s]
            for t in range(1, NTP):
                total += rcv[t, block + s]
            both.append(total * (1.0 / CH))
        return both

    def stage2(n, first, size):
        block, count = first // LANES, size // LANES
        activ = []
        for s, total in enumerate(totals(ex1_rcv, ex1_sem, block, count, n)):
            mean = total[0:1]
            inv = lax.rsqrt(total[1:2] - mean * mean + 1e-05)
            m, r = column(mean), column(inv)
            start = first + s * LANES
            rcol[pl.ds(pl.multiple_of(start, LANES), LANES), :] = r
            sums1, sums2, acts = [], [], [[] for _ in range(LT)]
            gains = [0.0] * LT
            for j in range(0, LANES, NB):
                rows = pl.ds(pl.multiple_of(start + j, NB), NB)
                s1, s2 = 0.0, 0.0
                for lt in range(LT):
                    gain = gain_s[0:1, lanes(lt)]
                    xhat = (conv_s[lt, rows, :] - m[j : j + NB]) * r[j : j + NB]
                    n_ = xhat * gain
                    g = sigmoid(n_)
                    acts[lt].append((n_ * g).astype(BF16))
                    ng = ag_s[lt, rows, :] * (g * (1.0 + n_ * (1.0 - g)))
                    xg = ng * gain
                    conv_s[lt, rows, :] = xhat
                    xg_s[lt, rows, :] = xg
                    s1, s2 = s1 + xg, s2 + xg * xhat
                    gains[lt] += folded(ng * xhat)
                sums1.append(s1)
                sums2.append(s2)
            for lt in range(LT):
                tacc[lt, KERNEL] += gains[lt]
            rows = (row_sums(jnp.concatenate(v, axis=0)) for v in (sums1, sums2))
            record(ex2_src, ex2_rcv, block + s, rows)
            activ.append([jnp.concatenate(v, axis=0) for v in acts])
        for peer in tp_peers:
            blocks = pl.ds(block, count)
            remote(ex2_src.at[blocks], ex2_rcv.at[x, blocks], ex2_sem, {"tp": peer}, n).start()
        for s in range(count):
            for lt in range(LT):
                at = pl.ds(pl.multiple_of(first + s * LANES, LANES), LANES)
                act_t[lanes(lt), at] = activ[s][lt].T

    def stage2_big(i, _):
        stage2(i, pl.multiple_of(LANES + i * R, LANES), R)
        return 0

    lax.fori_loop(0, BIG, stage2_big, 0)
    stage2(BIG, *chunks[BIG])
    stage2(BIG + 1, *chunks[BIG + 1])

    cgh = remote(cg_s.at[:, pl.ds(0, HALO), :], cgh_s, cgh_sem, preceding)

    def stage3(n):
        first, size = chunks[n]
        block, count = first // LANES, size // LANES
        for s, total in enumerate(totals(ex2_rcv, ex2_sem, block, count, n)):
            rows = pl.ds(first + s * LANES, LANES)
            mcol[rows, :] = column(total[0:1])
            ncol[rows, :] = column(total[1:2])
        for lt in range(LT):

            def taps_block(j, carry, lt=lt):
                at = pl.multiple_of(first + j * TB, TB)
                rows = pl.ds(at, TB)
                g = rcol[rows, :] * (
                    xg_s[lt, rows, :] - mcol[rows, :] - conv_s[lt, rows, :] * ncol[rows, :]
                )
                cg_s[lt, rows, :] = g
                carry = list(carry)
                for k, window in windows(glu_s, lt, at + 2, TB):
                    carry[k] += folded(g * window)
                return tuple(carry)

            sums = lax.fori_loop(
                0, size // TB, taps_block, tuple(jnp.zeros((8, LANES), F32) for _ in range(KERNEL))
            )
            for k in range(KERNEL):
                tacc[lt, k] += sums[k]

    def back_block(j, _):
        at = pl.multiple_of(j * RB, RB)
        rows = pl.ds(at, RB)
        for lt in range(LT):
            acc = jnp.zeros((RB, LANES), F32)
            for k, window in windows(cg_s, lt, at, RB):
                tap = KERNEL - 1 - k
                acc += taps_s[tap : tap + 1, lanes(lt)] * window
            s = sig_s[lt, rows, :]
            glu = glu_s[lt, pl.ds(pl.multiple_of(at + HALO, RB), RB), :]
            vg_ref[rows, lanes(lt)] = (acc * s).astype(BF16)
            gg_ref[rows, lanes(lt)] = (acc * glu * (1.0 - s)).astype(BF16)
        return 0

    def stage4(first, last):
        lax.fori_loop(first // RB, last // RB, back_block, 0)

    def summed(ref, n):
        total = ref[0].astype(F32)
        for i in range(1, n):
            total += ref[i].astype(F32)
        return total

    D = og_s.shape[1]
    H = D // 2
    Q = H // 2
    B = C // (NZ * NY)
    shape = (C, C)
    i = lax.broadcasted_iota(jnp.int32, shape, 0)
    j = lax.broadcasted_iota(jnp.int32, shape, 1)
    source = ((i // B) % NZ) * (NY * B) + (i // (B * NZ)) * B + i % B
    permutation = jnp.where(j == source, 1.0, 0.0).astype(BF16)
    act_p[...] = jnp.dot(permutation, act_t[...], preferred_element_type=F32).astype(BF16)

    def partial(owner, part):
        columns = pl.ds(pl.multiple_of(owner * H + part * Q, Q), Q)
        rows = (act_t, act_p)[part]
        return jnp.dot(rows[...], og_s[:, columns], preferred_element_type=F32) * FACTOR

    for part in range(2):
        pc_src[part] = partial(1 - c, part).astype(BF16)
    core_copy = remote(pc_src, pc_rcv, pc_sem, partner)
    core_copy.start()
    hear(2)
    for part in range(2):
        own_s[part] = partial(c, part)

    stage3(0)

    core_copy.wait()
    N = NZ
    ZB = C // N

    def both_ways(src, dst, sems, swapped):
        z_part, y_part = (1, 0) if swapped else (0, 1)
        for i in z_peers:
            remote(src(z_part, i), dst.at[z_part, z], sems, {"z": i}).start()
        for i in y_peers:
            remote(src(y_part, i), dst.at[y_part, y], sems, {"y": i}).start()

    def finish(dst, sems):
        sample = dst.at[:, pl.ds(0, N - 1)]
        remote(sample, sample, sems, partner).wait()

    for part in range(2):
        own = own_s[part] + pc_rcv[part].astype(F32)
        for i in range(N):
            p1_src[part, i] = own[i * ZB : (i + 1) * ZB].astype(BF16)
    both_ways(lambda part, i: p1_src.at[part, i], p1_rcv, p1_sem, False)
    p1_rcv[0, z] = p1_src[0, z]
    p1_rcv[1, y] = p1_src[1, y]

    for n in range(1, len(chunks)):
        stage3(n)
    cgh.start()

    S = KERNEL + 1
    A = S // 2
    for lt in range(LT):
        tc_src[:, lanes(lt)] = jnp.sum(tacc[lt], axis=1) * FACTOR
    taps_core = remote(tc_src, tc_rcv, tc_sem, partner)
    taps_swap = remote(ts_src, ts_rcv, ts_sem, partner)

    @pl.when(c == 0)
    def _():
        taps_core.start()

    stage4(0, R)

    @pl.when(c == 1)
    def _():
        taps_core.wait_recv()
        both = tc_src[...] + tc_rcv[...]
        t1_src[0] = both[0:A]
        t1_src[1] = both[A:S]
        both_ways(lambda part, i: t1_src.at[part], t1_rcv, t1_sem, False)
        t1_rcv[0, z] = both[0:A]
        t1_rcv[1, y] = both[A:S]

    stage4(R, T - R)
    cgh.wait()
    last = jnp.where(sp == NSP - 1, 0.0, 1.0).astype(F32)
    cg_s[:, pl.ds(T, HALO), :] = cgh_s[...] * last
    stage4(T - R, T)

    finish(p1_rcv, p1_sem)
    for part in range(2):
        sums = summed(p1_rcv.at[part], N)
        for i in range(N):
            p2_src[part, i] = sums[i * B : (i + 1) * B]
    both_ways(lambda part, i: p2_src.at[part, i], p2_rcv, p2_sem, True)
    p2_rcv[0, y] = p2_src[0, y]
    p2_rcv[1, z] = p2_src[1, z]

    @pl.when(c == 1)
    def _():
        finish(t1_rcv, t1_sem)
        half_a, half_b = summed(t1_rcv.at[0], N), summed(t1_rcv.at[1], N)
        t2_src[0] = half_a
        t2_src[1] = half_b
        both_ways(lambda part, i: t2_src.at[part], t2_rcv, t2_sem, True)
        t2_rcv[0, y] = half_a
        t2_rcv[1, z] = half_b

    finish(p2_rcv, p2_sem)
    done_a, done_b = summed(p2_rcv.at[0], N), summed(p2_rcv.at[1], N)
    CB = B // 2
    for i in range(2):
        ps_src[i, :, 0:Q] = done_a[i * CB : (i + 1) * CB]
        ps_src[i, :, Q:H] = done_b[i * CB : (i + 1) * CB]
    proj_swap = remote(ps_src.at[1 - c], ps_rcv, ps_sem, partner)
    proj_swap.start()

    @pl.when(c == 1)
    def _():
        finish(t2_rcv, t2_sem)
        ts_src[0:A] = summed(t2_rcv.at[0], N)
        ts_src[A:S] = summed(t2_rcv.at[1], N)
        taps_swap.start()
        tg_ref[...] = ts_src[0:KERNEL]
        ng_ref[...] = ts_src[KERNEL : KERNEL + 1]

    proj_swap.wait()
    mine, theirs = ps_src[c], ps_rcv[...]
    for i in range(2):
        proj_ref[:, i * H : (i + 1) * H] = jnp.where(c == i, mine, theirs)
    halo.wait_send()
    for rcv, sem in ((ex1_rcv, ex1_sem), (ex2_rcv, ex2_sem)):
        sample = rcv.at[pl.ds(0, NTP - 1)]
        remote(sample, sample, sem, partner).wait_send()

    @pl.when(c == 1)
    def _():
        taps_swap.wait_send()

    @pl.when(c == 0)
    def _():
        taps_core.wait_send()
        taps_swap.wait_recv()
        tg_ref[...] = ts_rcv[0:KERNEL]
        ng_ref[...] = ts_rcv[KERNEL : KERNEL + 1]


def store_kernel(*refs):
    n = len(refs) // 2
    sems = refs[-1]
    copies = [pltpu.make_async_copy(refs[i], refs[n + i], sems.at[i]) for i in range(n)]
    for copy in copies:
        copy.start()
    for copy in copies:
        copy.wait()


def per_device(sizes, glu_value, glu_gate, conv_taps, channel_gain, proj_weight, out_grad):
    NZ, NY, NTP = sizes
    T, C = glu_value.shape
    K = conv_taps.shape[0]
    D = out_grad.shape[1]
    LT, S, A = C // LANES, K + 1, (K + 1) // 2
    N, ZB, B = NZ, C // NZ, C // (NZ * NY)
    NBLK = T // LANES
    NCH = (T - 2 * LANES) // R + 2
    CB = B // 2
    H, Q = D // 2, D // 4
    factor = float(1.0 / (T * NZ * NY * 2) ** 0.5)
    params = (NZ, NY, NTP, T, C, K, C * NTP, factor)
    full = (LT, T, LANES)
    vmem, dma = pltpu.VMEM, pltpu.SemaphoreType.DMA
    any_spec = pl.BlockSpec(memory_space=pltpu.HBM)
    vmem_spec = pl.BlockSpec(memory_space=pltpu.VMEM)
    scratch = [
        vmem((T, C), BF16), vmem((T, C), BF16), vmem((K, C), F32), vmem((1, C), F32),
        vmem((C, D), BF16), vmem((T, D), BF16),
        vmem((2, HALO, C), BF16),
        vmem((LT, T + HALO, LANES), F32), vmem(full, F32), vmem(full, F32), vmem(full, F32), vmem(full, F32),
        vmem((C, T), BF16), vmem((C, T), BF16),
        vmem((T, LANES), F32), vmem((T, LANES), F32), vmem((T, LANES), F32),
        vmem((LT, T + HALO, LANES), F32), vmem((LT, HALO, LANES), F32),
        vmem((LT, S, 8, LANES), F32),
        vmem((NBLK, 2, LANES), F32), vmem((NTP, NBLK, 2, LANES), F32),
        vmem((NBLK, 2, LANES), F32), vmem((NTP, NBLK, 2, LANES), F32),
        vmem((2, C, Q), BF16), vmem((2, C, Q), BF16), vmem((2, C, Q), F32),
        vmem((2, N, ZB, Q), BF16), vmem((2, N, ZB, Q), BF16),
        vmem((2, N, B, Q), F32), vmem((2, N, B, Q), F32),
        vmem((2, CB, H), F32), vmem((CB, H), F32),
        vmem((S, C), F32), vmem((S, C), F32),
        vmem((2, A, C), F32), vmem((2, N, A, C), F32),
        vmem((2, A, C), F32), vmem((2, N, A, C), F32),
        vmem((S, C), F32), vmem((S, C), F32),
        dma((6,)), dma((2,)), dma((1 + NCH,)), dma((1 + NCH,)), dma((2,)),
    ] + [dma((2,))] * 8 + [pltpu.SemaphoreType.REGULAR((max(NY // 2 - 1, 1),))]
    results = (
        jax.ShapeDtypeStruct((T, C), BF16),
        jax.ShapeDtypeStruct((T, C), BF16),
        jax.ShapeDtypeStruct((CB, D), F32),
        jax.ShapeDtypeStruct((K, C), F32),
        jax.ShapeDtypeStruct((1, C), F32),
    )
    held = pl.pallas_call(
        functools.partial(kernel, params),
        out_shape=results,
        in_specs=[any_spec] * 6,
        out_specs=(vmem_spec,) * 5,
        scratch_shapes=scratch,
        compiler_params=pltpu.CompilerParams(
            collective_id=0, has_side_effects=True, vmem_limit_bytes=40 * 2**20
        ),
    )(*(
        pltpu.with_memory_space_constraint(a, pltpu.HBM)
        for a in (glu_value, glu_gate, conv_taps, channel_gain[None], proj_weight, out_grad)
    ))
    value_grad, gate_grad, proj_grad, taps_grad, gain_grad = pl.pallas_call(
        store_kernel,
        out_shape=results,
        in_specs=[vmem_spec] * 5,
        out_specs=(any_spec,) * 5,
        scratch_shapes=[dma((5,))],
        compiler_params=pltpu.CompilerParams(vmem_limit_bytes=8 * 2**20),
    )(*held)
    return value_grad, gate_grad, proj_grad, taps_grad, gain_grad[0]


def solution(mesh):
    return sized(mesh, 8, 8)


def sized(mesh, nz, ny):
    tp = mesh.shape["tp"]
    finer = Mesh(mesh.devices.reshape(nz, ny, 2, tp), ("z", "y", "c", "tp"))
    return jax.shard_map(
        functools.partial(per_device, (nz, ny, tp)),
        mesh=finer,
        in_specs=(P(SP, "tp"), P(SP, "tp"), P(None, "tp"), P("tp"), P("tp", None), P(SP, None)),
        out_specs=(P(SP, "tp"), P(SP, "tp"), P(TP_SP, None), P(None, "tp"), P("tp")),
        check_vma=False,
    )
```
